256 devices in a mesh: sp: 32 (over z, x), fs: 4 (over y), tp: 2 (over core).
Axes of the slice: x: 4, y: 4, z: 8, core: 2. Of those that a mesh axis runs over, the one named last changes fastest.
Arguments:
- tokens: bfloat16 [4, 8192, 2048], P('fs', ('sp', 'tp')), may hold values from -6 to 6
- norm_gain: float32 [2048], replicated, may hold values from 0.1 to 1.9
- w_query: bfloat16 [2048, 1024], P('fs', 'tp'), may hold values from -0.125 to 0.125
- w_key: bfloat16 [2048, 1024], P('fs', 'tp'), may hold values from -0.125 to 0.125
- w_value: bfloat16 [2048, 1024], P('fs', 'tp'), may hold values from -0.125 to 0.125
- w_conv_value: bfloat16 [2048, 1024], P('fs', 'tp'), may hold values from -2 to 2
- w_conv_gate: bfloat16 [2048, 1024], P('fs', 'tp'), may hold values from -0.125 to 0.125
- key_offset: bfloat16 [8192, 16], P('sp', 'tp'), may hold values from -16 to 2
- conv_kernel: float32 [31, 1024], P(None, 'tp'), may hold values from -3 to 3
- conv_gain: float32 [1024], P('tp'), may hold values from 0.1 to 1.9
- w_attn_out: bfloat16 [1024, 2048], P('tp', 'fs'), may hold values from -1 to 1
- w_conv_out: bfloat16 [1024, 2048], P('tp', 'fs'), may hold values from -0.1875 to 0.1875
Outputs:
- mixed: bfloat16 [4, 8192, 2048], P('fs', ('sp', 'tp'))
The draws below stay inside these ranges and needn't reach their ends.
All inputs are finite; a program needn't handle non-finite values.
Results may differ from the reference program's by a relative error of at most 0.0085.
Values may be sent and summed in bfloat16 or wider, within the bound.
A program may use at most 128 MiB of HBM per device.

```python
import math
import jax
import jax.numpy as jnp
from jax import lax

D = 2048
STICK_HEADS = 16
HD = 64
CC = 1024
KW = 31
TOK_DEV = 256
SBW = 1024
SEQUENCE_LENGTH = 8192
BATCH = 4
N_TP = 2


def draw_key_offset(key, part):
    divisions = jax.random.split(jax.random.fold_in(key, 11), 5)
    base_level = jax.random.uniform(divisions[0], (STICK_HEADS,), jnp.float32, -2.0, 5.0)
    block_shift = jax.random.uniform(divisions[1], (SEQUENCE_LENGTH // TOK_DEV, STICK_HEADS), jnp.float32, -0.8, 0.8)
    block_shift = jnp.repeat(block_shift, TOK_DEV, axis=0)
    roughness = jnp.clip(0.3 * jax.random.normal(divisions[2], (SEQUENCE_LENGTH, STICK_HEADS), jnp.float32), -1.0, 1.0)
    signal_height = base_level[None, :] - math.log(SEQUENCE_LENGTH) + block_shift + roughness
    spike_locations = jax.random.randint(divisions[3], (4,), 0, SEQUENCE_LENGTH)
    spike_flags = jnp.any(jnp.arange(SEQUENCE_LENGTH)[:, None] == spike_locations[None, :], axis=1)
    spike_magnitude = jax.random.uniform(divisions[4], (SEQUENCE_LENGTH, STICK_HEADS), jnp.float32, -1.2, 0.0)
    return jnp.where(spike_flags[:, None], spike_magnitude, signal_height).astype(jnp.bfloat16)


def draw_conv_kernel(key, part):
    divisions = jax.random.split(jax.random.fold_in(key, 23), 2)
    ramp = jnp.exp(jnp.linspace(math.log(0.4), math.log(2.0), CC)).astype(jnp.float32)
    entries = jnp.clip(jax.random.normal(divisions[0], (KW, CC), jnp.float32), -4.0, 4.0)
    common_tap = 0.1
    roughness = jax.random.uniform(divisions[1], (CC,), jnp.float32, 0.5, 1.5)
    return (entries * KW ** (-0.5) * ramp[None, :] * roughness[None, :] + common_tap).astype(jnp.float32)


def draw_w_conv_value(key, part):
    divisions = jax.random.split(jax.random.fold_in(key, 37), 3)
    levels = jnp.exp(jnp.linspace(math.log(0.3), math.log(3.0), CC)).astype(jnp.float32)
    noise = jnp.clip(jax.random.normal(divisions[0], (D, CC), jnp.float32), -4.0, 4.0)
    shared = jnp.clip(jax.random.normal(divisions[1], (D,), jnp.float32), -3.0, 3.0)
    roughness = jax.random.uniform(divisions[2], (CC,), jnp.float32, 0.7, 1.0)
    return ((noise + shared[:, None] * (levels * roughness)[None, :]) * D ** (-0.5)).astype(jnp.bfloat16)


def block_levels(stream_key, shape, pieces, smallest, top_value):
    def one(dim, blocks):
        heights = jax.random.uniform(jax.random.fold_in(jax.random.fold_in(stream_key, 6), dim), (blocks,), jnp.float32, smallest / len(pieces), top_value / len(pieces))
        return jnp.repeat(jnp.exp(heights), shape[dim] // blocks).reshape((-1,) + (1,) * (len(shape) - dim - 1))

    factor_of = one(*pieces[0])
    for cut in pieces[1:]:
        factor_of = factor_of * one(*cut)
    return factor_of


def bell_draw(own_key, extent, scale, limit, pieces=(), kind=jnp.bfloat16):
    gain = block_levels(own_key, extent, pieces, -0.22, 0.18) if pieces else 1.0
    values = jax.random.normal(own_key, extent, jnp.float32) * scale * gain
    return jnp.minimum(jnp.maximum(values, -limit), limit).astype(kind)


def setup_inputs(seed: int = 0) -> dict:
    streams_of = jax.random.split(jax.random.key(seed), 13)
    tokens = bell_draw(streams_of[0], (BATCH, SEQUENCE_LENGTH, D), 1.0, 6.0, ((0, 4), (1, 64)))
    norm_gain = jnp.clip(1.0 + 0.18 * jax.random.normal(streams_of[1], (D,), jnp.float32), 0.1, 1.9)
    w_query = bell_draw(streams_of[2], (D, SBW), D ** -0.5, 0.125, ((0, 4), (1, 2)))
    w_key = bell_draw(streams_of[3], (D, SBW), D ** -0.5, 0.125, ((0, 4), (1, 2)))
    w_value = bell_draw(streams_of[4], (D, SBW), D ** -0.5, 0.125, ((0, 4), (1, 2)))
    w_conv_value = draw_w_conv_value(jax.random.fold_in(streams_of[12], 71), 0)
    w_conv_gate = bell_draw(streams_of[6], (D, CC), D ** -0.5, 0.125, ((0, 4), (1, 2)))
    key_offset = draw_key_offset(jax.random.fold_in(streams_of[12], 71), 0)
    conv_kernel = draw_conv_kernel(jax.random.fold_in(streams_of[12], 71), 0)
    conv_gain = jnp.clip(1.0 + 0.18 * jax.random.normal(streams_of[9], (CC,), jnp.float32), 0.1, 1.9)
    w_attn_out = bell_draw(streams_of[10], (SBW, D), (SBW // 32) ** -0.5, 1.0, ((0, 2), (1, 4)))
    w_conv_out = bell_draw(streams_of[11], (CC, D), CC ** -0.5, 0.1875, ((0, 2), (1, 4)))
    return {"tokens": tokens, "norm_gain": norm_gain, "w_query": w_query, "w_key": w_key, "w_value": w_value, "w_conv_value": w_conv_value, "w_conv_gate": w_conv_gate, "key_offset": key_offset, "conv_kernel": conv_kernel, "conv_gain": conv_gain, "w_attn_out": w_attn_out, "w_conv_out": w_conv_out}


def reference(tokens, norm_gain, w_query, w_key, w_value, w_conv_value, w_conv_gate, key_offset, conv_kernel, conv_gain, w_attn_out, w_conv_out):
    floats = tokens.astype(jnp.float32)
    normed = (floats * lax.rsqrt(lax.optimization_barrier(jnp.mean(floats * floats, axis=2, keepdims=True)) + 1e-06) * norm_gain).astype(jnp.bfloat16)
    flat_rows = normed.reshape(BATCH * SEQUENCE_LENGTH, D)

    def project(weight):
        return jnp.dot(flat_rows, weight, preferred_element_type=jnp.float32).astype(jnp.bfloat16).reshape(BATCH, SEQUENCE_LENGTH, weight.shape[1])
    queries = project(w_query)
    key_rows = project(w_key)
    value_rows = project(w_value)
    conv_value = project(w_conv_value)
    conv_gate = project(w_conv_gate)
    offsets = jnp.transpose(key_offset.astype(jnp.float32))
    key_pos = jnp.arange(SEQUENCE_LENGTH, dtype=jnp.int32)
    blocks = SEQUENCE_LENGTH // TOK_DEV
    score_scale = HD ** (-0.5)

    def one_block(index):
        batch_index = index // blocks
        first_row = index % blocks * TOK_DEV
        seq_query = lax.dynamic_index_in_dim(queries, batch_index, 0, keepdims=False)
        query_block = lax.dynamic_slice_in_dim(seq_query, first_row, TOK_DEV, 0).reshape(TOK_DEV, STICK_HEADS, HD)
        seq_keys = lax.dynamic_index_in_dim(key_rows, batch_index, 0, keepdims=False).reshape(SEQUENCE_LENGTH, STICK_HEADS, HD)
        seq_values = lax.dynamic_index_in_dim(value_rows, batch_index, 0, keepdims=False).reshape(SEQUENCE_LENGTH, STICK_HEADS, HD)
        logits = jnp.einsum('qhd,khd->hqk', query_block.astype(jnp.float32), seq_keys.astype(jnp.float32)) * score_scale
        logits = logits + offsets[:, None, :]
        query_pos = first_row + jnp.arange(TOK_DEV, dtype=jnp.int32)
        allowed = key_pos[None, :] < query_pos[:, None]
        log_keep = jnp.where(allowed[None], jax.nn.log_sigmoid(-logits), 0.0)
        between = lax.cumsum(log_keep, axis=2, reverse=True) - log_keep
        weights = jnp.where(allowed[None], jnp.exp(jax.nn.log_sigmoid(logits) + between), 0.0).astype(jnp.bfloat16)
        result = jnp.einsum('hqk,khd->qhd', weights.astype(jnp.float32), seq_values.astype(jnp.float32))
        return result.reshape(TOK_DEV, SBW).astype(jnp.bfloat16)
    attn_heads = lax.map(one_block, jnp.arange(BATCH * blocks, dtype=jnp.int32)).reshape(BATCH, SEQUENCE_LENGTH, SBW)
    gated_input = (conv_value.astype(jnp.float32) * jax.nn.sigmoid(conv_gate.astype(jnp.float32))).astype(jnp.bfloat16)
    padded = jnp.pad(gated_input, ((0, 0), (KW - 1, 0), (0, 0))).astype(jnp.float32)
    conv_sum = jnp.zeros((BATCH, SEQUENCE_LENGTH, CC), jnp.float32)
    for tap_index in range(KW):
        conv_sum = conv_sum + conv_kernel[tap_index] * padded[:, tap_index:tap_index + SEQUENCE_LENGTH]
    mean_val = lax.optimization_barrier(jnp.mean(conv_sum, axis=2, keepdims=True))
    centred = conv_sum - mean_val
    spread = lax.optimization_barrier(jnp.mean(centred * centred, axis=2, keepdims=True))
    conv_hidden = jax.nn.silu(centred * lax.rsqrt(spread + 1e-06) * conv_gain).astype(jnp.bfloat16)
    head_cols = SBW // N_TP
    chan_cols = CC // N_TP
    attn_flat = attn_heads.reshape(BATCH * SEQUENCE_LENGTH, SBW)
    conv_flat = conv_hidden.reshape(BATCH * SEQUENCE_LENGTH, CC)
    total = jnp.zeros((BATCH * SEQUENCE_LENGTH, D), jnp.float32)
    for group in range(N_TP):
        partial_value = jnp.dot(attn_flat[:, group * head_cols:(group + 1) * head_cols], w_attn_out[group * head_cols:(group + 1) * head_cols], preferred_element_type=jnp.float32)
        partial_value = partial_value + jnp.dot(conv_flat[:, group * chan_cols:(group + 1) * chan_cols], w_conv_out[group * chan_cols:(group + 1) * chan_cols], preferred_element_type=jnp.float32)
        total = total + lax.optimization_barrier(partial_value.astype(jnp.bfloat16)).astype(jnp.float32)
    return total.astype(jnp.bfloat16).reshape(BATCH, SEQUENCE_LENGTH, D)
```

```python
import functools
import math

import jax
import jax.numpy as jnp
from jax import lax
from jax.experimental import pallas as pl
from jax.experimental.pallas import tpu as pltpu
from jax.sharding import Mesh
from jax.sharding import PartitionSpec as P

MESH = pl.DeviceIdType.MESH
F32 = jnp.float32
BF16 = jnp.bfloat16
LOG2E = math.log2(math.e)
TOP = 25.0
HD = 64
CC = 1024
KW = 31
UNIT = 1024
QB = 256
NZ = 8
NX = 4
EDGE = 32
VM = pl.BlockSpec(memory_space=pltpu.VMEM)
ANY = pl.BlockSpec(memory_space=pl.ANY)


def sems(*counts):
    return [pltpu.SemaphoreType.DMA((n,)) for n in counts]


def remote(src, dst, send, recv, **to):
    return pltpu.make_async_remote_copy(
        src_ref=src, dst_ref=dst, send_sem=send, recv_sem=recv, device_id=to, device_id_type=MESH
    )


def signal(**to):
    pl.semaphore_signal(
        pltpu.get_barrier_semaphore(), inc=1, device_id=to, device_id_type=MESH
    )


class Ring:
    def __init__(self, axis, me, at, send, recv):
        right, left = lax.rem(me + 1, 4), lax.rem(me + 3, 4)
        self.left, self.right = left, right

        def hop(block, half, slot, to):
            ref = at(block, half)
            return remote(ref, ref, send.at[slot], recv.at[slot], **{axis: to})

        self.first = [hop(me, 0, 0, right), hop(me, 1, 2, left), hop(me, 1, 1, right), hop(me, 0, 3, left)]
        self.second = [hop(left, 0, 4, right), hop(right, 1, 5, left)]

    def start(self):
        for copy in self.first:
            copy.start()

    def forward(self):
        for got, copy in zip(self.first[:2], self.second):
            got.wait_recv()
            copy.start()

    def neighbours(self):
        for copy in self.first[2:]:
            copy.wait_recv()

    def far(self):
        for copy in self.second:
            copy.wait_recv()

    def sent(self):
        for copy in self.first + self.second:
            copy.wait_send()


def collect_kernel(tok, gain, off, wq, wk, wv, wcv, wcg, rows, weights, offs, ws, xs, xr, ys, yr, ds, dr, os_, or_):
    x, y, c = (lax.axis_index(n) for n in ("x", "fs", "tp"))
    loads = [
        pltpu.make_async_copy(
            w.at[:, pl.ds(pl.multiple_of(x * 128, 128), 128)], weights.at[y, :, pl.ds(i * 128, 128)], ws.at[i]
        )
        for i, w in enumerate((wq, wk, wv, wcv, wcg))
    ]
    for load in loads:
        load.start()
    for d in (1, 2, 3):
        signal(x=lax.rem(x + d, 4))
    signal(fs=lax.rem(y + 1, 4))
    signal(fs=lax.rem(y + 3, 4))
    signal(tp=1 - c)

    def norm(i, _):
        at = pl.ds(pl.multiple_of(i * 16, 16), 16)
        floats = tok[at, :].astype(F32)
        scale = lax.rsqrt(jnp.mean(floats * floats, axis=1, keepdims=True) + 1e-06)
        rows[x, c, at, :] = (floats * scale * gain[...]).astype(BF16)
        return 0

    lax.fori_loop(0, 8, norm, 0)
    offs[x] = off[x]
    for load in loads:
        load.wait()
    pl.semaphore_wait(pltpu.get_barrier_semaphore(), 6)
    ring_y = Ring("fs", y, lambda b, h: weights.at[b, pl.ds(h * 256, 256)], ys, yr)
    ring_x = Ring("x", x, lambda b, h: rows.at[b, c, pl.ds(h * 64, 64)], xs, xr)

    def over(block, slot):
        ref = rows.at[block, c]
        return remote(ref, ref, ds.at[slot], dr.at[slot], tp=1 - c)

    across = [over(x, 0), over(ring_x.left, 1), over(ring_x.right, 2), over(lax.rem(x + 2, 4), 3)]
    ring_y.start()
    ring_x.start()
    across[0].start()
    small = [
        remote(off.at[lax.rem(x + d, 4)], offs.at[x], os_.at[d - 1], or_.at[d - 1], x=lax.rem(x + d, 4))
        for d in (1, 2, 3)
    ]
    for copy in small:
        copy.start()
    ring_x.forward()
    ring_y.forward()
    ring_x.neighbours()
    across[1].start()
    across[2].start()
    ring_x.far()
    across[3].start()
    for copy in small:
        copy.wait()
    ring_y.neighbours()
    ring_y.far()
    for copy in across:
        copy.wait()
    ring_x.sent()
    ring_y.sent()


def collect(tokens, gain, off, ws):
    return pl.pallas_call(
        collect_kernel,
        out_shape=(
            jax.ShapeDtypeStruct((NX, 2, 128, 2048), BF16),
            jax.ShapeDtypeStruct((4, 512, 640), BF16),
            jax.ShapeDtypeStruct((NX, 2, 8, 128), F32),
        ),
        in_specs=[VM, VM, VM] + [ANY] * 5,
        out_specs=(VM, VM, VM),
        scratch_shapes=sems(5, 6, 6, 6, 6, 4, 4, 3, 3),
        compiler_params=pltpu.CompilerParams(
            collective_id=1, has_side_effects=True, vmem_limit_bytes=40 * 2**20
        ),
        name="collect",
    )(tokens, gain, off, *ws)


def project_kernel(rows, weights, offs, qt, kp, vt, m, gated, kf, vf, vp):
    def block(b, _):
        at = pl.ds(pl.multiple_of(b * 256, 256), 256)
        total = None
        for f in range(4):
            part = jnp.dot(rows[at, pl.ds(f * 512, 512)], weights[f], preferred_element_type=F32)
            total = part if total is None else total + part
        kf[at, :] = total[:, 128:256]
        vf[at, :] = total[:, 256:384]
        q = total[:, :128].T
        qt[0, b] = q[:64].astype(BF16)
        qt[1, b] = q[64:].astype(BF16)
        value = total[:, 384:512].astype(BF16).astype(F32)
        gate = total[:, 512:640].astype(BF16).astype(F32)
        gated[at, :] = (value / (1.0 + jnp.exp(-gate))).astype(BF16)
        return 0

    lax.fori_loop(0, 4, block, 0)
    low = lax.broadcasted_iota(jnp.int32, (8, 128), 1) < 64

    def keys(i, _):
        ks = [[], []]
        for s in (0, 1):
            near = kf[pl.ds(2 * i + s, 8, stride=128), :]
            later = kf[pl.ds(2 * i + s + 64, 8, stride=128), :]
            ks[0].append(jnp.where(low, near, pltpu.roll(later, 64, 1)))
            ks[1].append(jnp.where(low, pltpu.roll(near, 64, 1), later))
        at = pl.ds(pl.multiple_of(i * 16, 16), 16)
        for j in (0, 1):
            kp[j, at, :] = jnp.concatenate(ks[j], axis=0).astype(BF16)
        return 0

    lax.fori_loop(0, 32, keys, 0, unroll=4)

    def values(i, _):
        vp[pl.ds(pl.multiple_of(i * 8, 8), 8), :] = vf[pl.ds(i, 8, stride=128), :]
        return 0

    lax.fori_loop(0, 128, values, 0, unroll=8)
    for b in range(8):
        v = vp[pl.ds(b * 128, 128), :].T.astype(BF16)
        vt[0, :, pl.ds(b * 128, 128)] = v[:64]
        vt[1, :, pl.ds(b * 128, 128)] = v[64:]
    sub = lax.broadcasted_iota(jnp.int32, (8, 128), 0)
    for j in (0, 1):
        tile = offs[0, j]
        for x in (1, 2, 3):
            tile = jnp.where(sub < 2 * x, tile, pltpu.roll(offs[x, j], 2 * x, 0))
        m[j] = tile


def project(rows, weights, offs):
    return pl.pallas_call(
        project_kernel,
        out_shape=(
            jax.ShapeDtypeStruct((2, 4, HD, QB), BF16),
            jax.ShapeDtypeStruct((2, 512, 128), BF16),
            jax.ShapeDtypeStruct((2, HD, UNIT), BF16),
            jax.ShapeDtypeStruct((2, 8, 128), F32),
            jax.ShapeDtypeStruct((UNIT, 128), BF16),
        ),
        in_specs=[VM] * 3,
        out_specs=(VM,) * 5,
        scratch_shapes=[pltpu.VMEM((UNIT, 128), F32)] * 3,
        compiler_params=pltpu.CompilerParams(vmem_limit_bytes=40 * 2**20),
        name="project",
    )(rows.reshape(UNIT, 2048), weights, offs)


def exchange_kernel(
    qt, kp, vt, m, gated, wa, wc, kin, vin, qin, min_, gin, wout,
    wl, ys, yr, zs, ks, vs, qs, ms, ds, dr, xs, xr, hs, hr,
):
    z, x, y, c = (lax.axis_index(n) for n in ("z", "x", "fs", "tp"))
    loads = [pltpu.make_async_copy(w, wout.at[y, i], wl.at[i]) for i, w in enumerate((wa, wc))]
    for load in loads:
        load.start()
    home = z // 4
    here = home == c
    order = [0, 1, 7, 2, 6, 3, 5, 4]
    for d in order:
        if d == 0:
            pl.when(jnp.logical_not(here))(lambda: signal(tp=1 - c))
        else:
            signal(z=lax.rem(z + d, 8), tp=home)
    signal(tp=1 - c)
    for d in (1, 2, 3):
        signal(x=lax.rem(x + d, 4))
    signal(fs=lax.rem(y + 1, 4))
    signal(fs=lax.rem(y + 3, 4))
    heir = jnp.logical_and(x == 0, z > 0)

    @pl.when(heir)
    def _():
        for s in range(4):
            signal(z=z - 1, x=s)

    @pl.when(jnp.logical_and(x == 0, z == 0))
    def _():
        for s in range(4):
            gin[s, pl.ds(0, EDGE), :] = jnp.zeros((EDGE, 128), BF16)

    for load in loads:
        load.wait()
    giver = z < 7
    pl.semaphore_wait(
        pltpu.get_barrier_semaphore(),
        14 - here.astype(jnp.int32) + giver.astype(jnp.int32),
    )

    sends = []

    def send(src, dst, slot, recv, zd, cd):
        same = jnp.logical_and(zd == z, cd == c)
        copy = remote(src, dst, zs.at[slot], recv, z=zd, tp=cd)

        @pl.when(same)
        def _():
            pltpu.make_async_copy(src, dst, recv).start()

        @pl.when(jnp.logical_not(same))
        def _():
            copy.start()

        sends.append((jnp.logical_not(same), copy))

    odd = lax.rem(z, 2)
    for jj in range(4):
        zd, j, half = 4 * c + jj, jj // 2, jj % 2
        send(kp.at[j], kin.at[z], 6 * jj, ks.at[z], zd, 0)
        send(vt.at[j], vin.at[z], 6 * jj + 1, vs.at[z], zd, 1)
        for cd in (0, 1):
            quarter = 2 * half + cd
            block = quarter + odd * (3 - 2 * quarter)
            send(qt.at[j, block], qin.at[z], 6 * jj + 2 + cd, qs.at[z], zd, cd)
            send(m.at[j], min_.at[z], 6 * jj + 4 + cd, ms.at[z], zd, cd)

    ring_y = Ring("fs", y, lambda b, h: wout.at[b, h], ys, yr)
    ring_y.start()

    def part(to):
        return gated.at[pl.ds(pl.multiple_of(to * 256 - EDGE, EDGE), 256 + EDGE), :]

    own = pltpu.make_async_copy
    rows_x = []
    for d in (1, 2, 3):
        to = lax.rem(x + d, 4)
        whole = remote(part(to), gin.at[x], xs.at[d - 1], xr.at[x], x=to)
        less = remote(
            gated.at[pl.ds(0, 256), :], gin.at[x, pl.ds(EDGE, 256), :], xs.at[d - 1], xr.at[x], x=to
        )
        pl.when(to > 0)(whole.start)
        pl.when(to == 0)(less.start)
        rows_x.append((to, whole, less))
    own_whole = own(part(x), gin.at[x], xr.at[x])
    own_less = own(gated.at[pl.ds(0, 256), :], gin.at[x, pl.ds(EDGE, 256), :], xr.at[x])
    pl.when(x > 0)(own_whole.start)
    pl.when(x == 0)(own_less.start)
    edge = remote(
        gated.at[pl.ds(UNIT - EDGE, EDGE), :], gin.at[x, pl.ds(0, EDGE), :], hs.at[0], hr.at[x], z=z + 1, x=0
    )
    pl.when(giver)(edge.start)

    def pass_on(at, source):
        ref, sem = (kin, ks) if at == 0 else (vin, vs)
        return remote(ref.at[source], ref.at[source], ds.at[source], sem.at[source], tp=1 - at)

    for core in (0, 1):
        @pl.when(c == core)
        def _(core=core):
            for n, d in enumerate(order):
                source = lax.rem(z + d, 8)
                copy = pass_on(core, source)
                copy.wait_recv()
                copy.start()
                if n == 4:
                    ring_y.forward()
            for d in order:
                source = lax.rem(z + d, 8)
                pass_on(1 - core, source).wait_recv()
                pass_on(core, source).wait_send()

    for d in order:
        source = lax.rem(z + d, 8)
        pltpu.make_async_copy(qt.at[0, 0], qin.at[source], qs.at[source]).wait()
        pltpu.make_async_copy(m.at[0], min_.at[source], ms.at[source]).wait()
    for s in range(4):
        pl.when(x > 0)(own(part(1), gin.at[s], xr.at[s]).wait)
        pl.when(x == 0)(own(gated.at[pl.ds(0, 256), :], gin.at[s, pl.ds(EDGE, 256), :], xr.at[s]).wait)
        pl.when(heir)(own(gated.at[pl.ds(0, EDGE), :], gin.at[s, pl.ds(0, EDGE), :], hr.at[s]).wait)
    for cond, copy in sends:
        pl.when(cond)(copy.wait_send)
    for to, whole, less in rows_x:
        pl.when(to > 0)(whole.wait_send)
        pl.when(to == 0)(less.wait_send)
    pl.when(giver)(edge.wait_send)
    ring_y.neighbours()
    ring_y.far()
    ring_y.sent()


def exchange(qt, kp, vt, m, gated, wa, wc):
    return pl.pallas_call(
        exchange_kernel,
        out_shape=(
            jax.ShapeDtypeStruct((NZ, 512, 128), BF16),
            jax.ShapeDtypeStruct((NZ, HD, UNIT), BF16),
            jax.ShapeDtypeStruct((NZ, HD, QB), BF16),
            jax.ShapeDtypeStruct((NZ, 8, 128), F32),
            jax.ShapeDtypeStruct((NX, 256 + EDGE, 128), BF16),
            jax.ShapeDtypeStruct((4, 2, 512, 512), BF16),
        ),
        in_specs=[VM] * 5 + [ANY] * 2,
        out_specs=(VM,) * 6,
        scratch_shapes=sems(2, 6, 6, 24, 8, 8, 8, 8, 8, 8, 3, 4, 1, 4),
        compiler_params=pltpu.CompilerParams(
            collective_id=2, has_side_effects=True, vmem_limit_bytes=40 * 2**20
        ),
        name="exchange",
    )(qt, kp, vt, m, gated, wa, wc)


def suffix(t):
    sub = lax.broadcasted_iota(jnp.int32, t.shape, 0)
    e = jnp.where(sub < 7, pltpu.roll(t, 7, 0), 1.0)
    for step in (1, 2, 4):
        e = e * jnp.where(sub < 8 - step, pltpu.roll(e, 8 - step, 0), 1.0)
    return e


def weigh(s_ref, cap, r_ref, w_ref, carry, first):
    t = None
    for g in range(31, -1, -1):
        d = []
        for j in range(4):
            rows = pl.ds((4 * g + j) * 8, 8)
            e = jnp.exp2(jnp.minimum(s_ref[rows, :] * LOG2E, cap[rows, :]))
            s_ref[rows, :] = e
            d.append(e + 1.0)
        r = 1.0 / ((d[0] * d[1]) * (d[2] * d[3]))
        r_ref[pl.ds(g * 8, 8), :] = r
        t = r if t is None else t * r
    start = jnp.where(first, 1.0, carry[...])
    p = suffix(t) * start
    carry[...] = jnp.broadcast_to((p * t)[0:1, :], p.shape)
    for g in range(31, -1, -1):
        e = [s_ref[pl.ds((4 * g + j) * 8, 8), :] for j in range(4)]
        p = p * r_ref[pl.ds(g * 8, 8), :]
        p1 = p * (e[0] + 1.0)
        p2 = p1 * (e[1] + 1.0)
        p3 = p2 * (e[2] + 1.0)
        w = jnp.concatenate([e[0] * p, e[1] * p1, e[2] * p2, e[3] * p3], axis=0)
        w_ref[pl.ds(g * 32, 32), :] = w.astype(BF16)


def attend_kernel(q_ref, k_ref, v_ref, m_ref, o_ref, qa, qb, off, s0, s1, w0, w1, r_ref, cap, carry, acc):
    z, c = lax.axis_index("z"), lax.axis_index("tp")
    quarter = 2 * lax.rem(z, 2) + c
    zero = jnp.zeros((HD, QB), BF16)
    row = lax.broadcasted_iota(jnp.int32, (128, QB), 0)
    one_a, one_b = ((row == i).astype(F32).astype(BF16) for i in (0, 1))

    def prepare(i, _):
        q = (q_ref[i].astype(F32) * 0.125).astype(BF16)
        qa[i] = jnp.concatenate([q, zero, one_a], axis=0)
        qb[i] = jnp.concatenate([zero, q, one_b], axis=0)
        tile = m_ref[i]
        col = lax.broadcasted_iota(jnp.int32, (8, 128), 1)
        for pair in range(32):
            both = []
            for n in (2 * pair, 2 * pair + 1):
                near = jnp.broadcast_to(tile[:, n : n + 1], (8, 128))
                later = jnp.broadcast_to(tile[:, n + 64 : n + 65], (8, 128))
                both.append(jnp.where(col == 0, near, jnp.where(col == 1, later, 0.0)))
            off[i, pl.ds(pair * 16, 16), :] = jnp.concatenate(both, axis=0).astype(BF16)
        return 0

    lax.fori_loop(0, NZ, prepare, 0)
    lane = lax.broadcasted_iota(jnp.int32, (8, QB), 1)
    sub = lax.broadcasted_iota(jnp.int32, (8, QB), 0)

    def caps(i, _):
        key = sub * 128 + i
        rows = pl.ds(pl.multiple_of(i * 8, 8), 8)
        cap[0, rows, :] = jnp.full((8, QB), TOP, F32)
        cap[1, rows, :] = jnp.where(key < lane + quarter * QB, TOP, -300.0)
        cap[2, rows, :] = jnp.where(key < lane + (3 - quarter) * QB, TOP, -300.0)
        return 0

    lax.fori_loop(0, 128, caps, 0, unroll=4)

    def following(u):
        zq, zk = u
        ends = zk == 0
        return (jnp.where(ends, zq + 1, zq), jnp.where(ends, zq + 1, zk - 1))

    def scores(u, s_ref):
        zq, zk = jnp.minimum(u[0], NZ - 1), jnp.minimum(u[1], NZ - 1)
        lhs = jnp.concatenate([k_ref[zk], off[zk]], axis=1)
        s_ref[0:512, :] = jnp.dot(lhs, qa[zq], preferred_element_type=F32)
        s_ref[512:1024, :] = jnp.dot(lhs, qb[zq], preferred_element_type=F32)

    def weights(u, s_ref, w_ref):
        zq, zk = u
        diagonal = zq == zk
        weigh(s_ref, cap.at[jnp.where(diagonal, 1 + lax.rem(zq, 2), 0)], r_ref, w_ref, carry, diagonal)

    def values(u, w_ref):
        zq, zk = u
        out = jnp.dot(v_ref[zk], w_ref[...], preferred_element_type=F32)
        acc[zq] = jnp.where(zq == zk, 0.0, acc[zq]) + out

    start = jnp.int32(0)
    carry[...] = jnp.ones_like(carry)
    w1[...] = jnp.zeros_like(w1)
    acc[0] = jnp.zeros_like(acc[0])
    scores((start, start), s0)

    def pair(_, state):
        before, now = state
        after = following(now)
        scores(after, s1)
        weights(now, s0, w0)
        values(before, w1)
        last = following(after)
        scores(last, s0)
        weights(after, s1, w1)
        values(now, w0)
        return (after, last)

    last, _ = lax.fori_loop(0, NZ * (NZ + 1) // 4, pair, ((start, start), (start, start)))
    values(last, w1)

    def finish(i, _):
        o_ref[i] = acc[i].astype(BF16)
        return 0

    lax.fori_loop(0, NZ, finish, 0)


def attend(q, k, v, m):
    return pl.pallas_call(
        attend_kernel,
        out_shape=jax.ShapeDtypeStruct((NZ, HD, QB), BF16),
        in_specs=[VM] * 4,
        out_specs=VM,
        scratch_shapes=[
            pltpu.VMEM((NZ, 256, QB), BF16),
            pltpu.VMEM((NZ, 256, QB), BF16),
            pltpu.VMEM((NZ, 512, 128), BF16),
            pltpu.VMEM((UNIT, QB), F32),
            pltpu.VMEM((UNIT, QB), F32),
            pltpu.VMEM((UNIT, QB), BF16),
            pltpu.VMEM((UNIT, QB), BF16),
            pltpu.VMEM((256, QB), F32),
            pltpu.VMEM((3, UNIT, QB), F32),
            pltpu.VMEM((8, QB), F32),
            pltpu.VMEM((NZ, HD, QB), F32),
        ],
        compiler_params=pltpu.CompilerParams(vmem_limit_bytes=48 * 2**20),
        name="attend",
    )(q, k, v, m)


def hand_back_kernel(o, oin, ss, rs):
    z, x, c = (lax.axis_index(n) for n in ("z", "x", "tp"))
    home = z // 4
    quarter = 2 * lax.rem(z, 2) + c
    head = 2 * x + lax.rem(z // 2, 2)
    wanted = x + lax.rem(z, 2) * (3 - 2 * x)
    for h in range(8):
        zs, xs, cs = 4 * c + 2 * (h % 2) + wanted // 2, h // 2, lax.rem(wanted, 2)
        self_ = jnp.logical_and(jnp.logical_and(zs == z, xs == x), cs == c)
        pl.when(jnp.logical_not(self_))(lambda zs=zs, xs=xs, cs=cs: signal(z=zs, x=xs, tp=cs))
    copies = []
    mine = jnp.int32(0)
    for zq in range(NZ):
        xd = quarter if zq % 2 == 0 else 3 - quarter
        self_ = jnp.logical_and(jnp.logical_and(z == zq, xd == x), home == c)
        mine = mine + self_.astype(jnp.int32)
        copies.append(
            (self_, remote(o.at[zq], oin.at[head], ss.at[zq], rs.at[head], z=zq, x=xd, tp=home), zq)
        )
    pl.semaphore_wait(pltpu.get_barrier_semaphore(), 8 - mine)
    for self_, copy, zq in copies:
        pl.when(jnp.logical_not(self_))(copy.start)
        pl.when(self_)(pltpu.make_async_copy(o.at[zq], oin.at[head], rs.at[head]).start)
    for h in range(8):
        pltpu.make_async_copy(o.at[0], oin.at[h], rs.at[h]).wait()
    for self_, copy, zq in copies:
        pl.when(jnp.logical_not(self_))(copy.wait_send)


def hand_back(o):
    return pl.pallas_call(
        hand_back_kernel,
        out_shape=jax.ShapeDtypeStruct((8, HD, QB), BF16),
        in_specs=[VM],
        out_specs=VM,
        scratch_shapes=sems(8, 8),
        compiler_params=pltpu.CompilerParams(collective_id=3, has_side_effects=True),
        name="hand_back",
    )(o)


def shards(
    tokens, norm_gain, w_query, w_key, w_value, w_conv_value, w_conv_gate,
    key_offset, conv_kernel, conv_gain, w_attn_out, w_conv_out,
):
    tile = key_offset.astype(F32).T.reshape(NX, 2, 2, 128)
    tile = jnp.pad(tile, ((0, 0), (0, 0), (0, 6), (0, 0)))
    rows, weights, offs = collect(
        tokens[0], norm_gain[None], tile, (w_query, w_key, w_value, w_conv_value, w_conv_gate)
    )
    qt, kp, vt, m, gated = project(rows, weights, offs)
    kin, vin, qin, min_, gin, wout = exchange(qt, kp, vt, m, gated, w_attn_out, w_conv_out)
    o = attend(qin, kin, vin, min_)
    heads = hand_back(o).reshape(512, QB)

    extended = jnp.moveaxis(gin, 0, 1).reshape(256 + EDGE, 512).astype(F32)
    conv_sum = jnp.zeros((256, 512), F32)
    for tap in range(KW):
        at = EDGE - (KW - 1) + tap
        conv_sum = conv_sum + conv_kernel[tap] * extended[at : at + 256]
    sums = jnp.stack([jnp.sum(conv_sum, axis=1), jnp.sum(conv_sum * conv_sum, axis=1)])
    sums = lax.all_gather(sums, "tp").sum(0)
    mean = sums[0] / CC
    spread = sums[1] / CC - mean * mean
    hidden = jax.nn.silu(
        (conv_sum - mean[:, None]) * lax.rsqrt(spread + 1e-06)[:, None] * conv_gain
    ).astype(BF16)

    wo = jnp.moveaxis(wout, 0, 2).reshape(2, 512, 2048)
    partial = lax.dot_general(heads, wo[0], (((0,), (0,)), ((), ())), preferred_element_type=F32)
    partial = partial + jnp.dot(hidden, wo[1], preferred_element_type=F32)
    parts = lax.optimization_barrier(partial.astype(BF16)).reshape(2, 128, 2048)
    arrived = lax.all_to_all(parts, "tp", split_axis=0, concat_axis=0, tiled=True)
    return arrived.astype(F32).sum(axis=0).astype(BF16)[None]


def solution(mesh):
    view = Mesh(mesh.devices.reshape(NZ, NX, 4, 2), ("z", "x", "fs", "tp"))
    rows = P("fs", ("z", "x", "tp"), None)
    placed = (
        rows, P(), P("fs", "tp"), P("fs", "tp"), P("fs", "tp"), P("fs", "tp"), P("fs", "tp"),
        P(("z", "x"), "tp"), P(None, "tp"), P("tp"), P("tp", "fs"), P("tp", "fs"),
    )
    return jax.shard_map(shards, mesh=view, in_specs=placed, out_specs=rows, check_vma=False)
```

```python
import functools
import math

import jax
import jax.numpy as jnp
from jax import lax
from jax.experimental import pallas as pl
from jax.experimental.pallas import tpu as pltpu
from jax.sharding import Mesh
from jax.sharding import PartitionSpec as P

MESH = pl.DeviceIdType.MESH
F32 = jnp.float32
BF16 = jnp.bfloat16
LOG2E = math.log2(math.e)
TOP = 25.0
HD = 64
CC = 1024
KW = 31
UNIT = 1024
QB = 256
NZ = 8
NX = 4
EDGE = 32
VM = pl.BlockSpec(memory_space=pltpu.VMEM)
HBM = pl.BlockSpec(memory_space=pltpu.HBM)


def sems(*counts):
    return [pltpu.SemaphoreType.DMA((n,)) for n in counts]


def remote(src, dst, send, recv, **to):
    return pltpu.make_async_remote_copy(
        src_ref=src, dst_ref=dst, send_sem=send, recv_sem=recv, device_id=to, device_id_type=MESH
    )


def signal(**to):
    pl.semaphore_signal(
        pltpu.get_barrier_semaphore(), inc=1, device_id=to, device_id_type=MESH
    )


class Ring:
    def __init__(self, axis, me, at, send, recv):
        right, left = lax.rem(me + 1, 4), lax.rem(me + 3, 4)
        self.left, self.right = left, right

        def hop(block, half, slot, to):
            ref = at(block, half)
            return remote(ref, ref, send.at[slot], recv.at[slot], **{axis: to})

        self.first = [hop(me, 0, 0, right), hop(me, 1, 2, left), hop(me, 1, 1, right), hop(me, 0, 3, left)]
        self.second = [hop(left, 0, 4, right), hop(right, 1, 5, left)]

    def start(self):
        for copy in self.first:
            copy.start()

    def forward(self):
        for got, copy in zip(self.first[:2], self.second):
            got.wait_recv()
            copy.start()

    def neighbours(self):
        for copy in self.first[2:]:
            copy.wait_recv()

    def far(self):
        for copy in self.second:
            copy.wait_recv()

    def sent(self):
        for copy in self.first + self.second:
            copy.wait_send()


def suffix(t):
    sub = lax.broadcasted_iota(jnp.int32, t.shape, 0)
    e = jnp.where(sub < 7, pltpu.roll(t, 7, 0), 1.0)
    for step in (1, 2, 4):
        e = e * jnp.where(sub < 8 - step, pltpu.roll(e, 8 - step, 0), 1.0)
    return e


def weigh(s_ref, cap, r_ref, w_ref, left):
    t = None
    for g in range(31, -1, -1):
        d = []
        for j in range(4):
            rows = pl.ds((4 * g + j) * 8, 8)
            e = jnp.exp2(jnp.minimum(s_ref[rows, :] * LOG2E, cap[rows, :]))
            s_ref[rows, :] = e
            d.append(e + 1.0)
        r = 1.0 / ((d[0] * d[1]) * (d[2] * d[3]))
        r_ref[pl.ds(g * 8, 8), :] = r
        t = r if t is None else t * r
    p = suffix(t)
    left[...] = jnp.broadcast_to((p * t)[0:1, :], p.shape)
    for g in range(31, -1, -1):
        e = [s_ref[pl.ds((4 * g + j) * 8, 8), :] for j in range(4)]
        p = p * r_ref[pl.ds(g * 8, 8), :]
        p1 = p * (e[0] + 1.0)
        p2 = p1 * (e[1] + 1.0)
        p3 = p2 * (e[2] + 1.0)
        w = jnp.concatenate([e[0] * p, e[1] * p1, e[2] * p2, e[3] * p3], axis=0)
        w_ref[pl.ds(g * 32, 32), :] = w.astype(BF16)


def nth(n):
    half = n // 2
    return jnp.where(lax.rem(n, 2) == 1, 4 - half, lax.rem(8 - half, 8))


def layer_kernel(
    tok, tok_gain, offx, taps, gain, wq, wk, wv, wcv, wcg, wa, wc, out_ref,
    rows, weights, offs, full, kf, vf, vp, qt, kp, vt, m, gated,
    kin, vin, qin, min_, gin, wout, ext, csum, stat, stat_in, hidden, heads, own_part, part_out, part_in,
    qa, qb, off, s0, s1, w0, w1, r_ref, cap, left, acc, oout, oin,
    ws, cxs, cxr, cys, cyr, cds, cdr, cos, cor,
    wl, ys, yr, zs, ks, vs, qs, ms, ds, dr, xs, xr, hs, hr, ss, sr, os_, or_, ps, pr,
):
    z, x, y, c = (lax.axis_index(n) for n in ("z", "x", "fs", "tp"))
    first_loads = [
        pltpu.make_async_copy(
            w.at[:, pl.ds(pl.multiple_of(x * 128, 128), 128)], weights.at[y, :, pl.ds(i * 128, 128)], ws.at[i]
        )
        for i, w in enumerate((wq, wk, wv, wcv, wcg))
    ]
    loads = [pltpu.make_async_copy(w, wout.at[y, i], wl.at[i]) for i, w in enumerate((wa, wc))]
    for load in first_loads + loads:
        load.start()
    home = z // 4
    here = home == c
    other = jnp.logical_not
    local = pltpu.make_async_copy
    for d in range(8):
        if d == 0:
            pl.when(other(here))(lambda: signal(tp=1 - c))
        else:
            signal(z=lax.rem(z + d, 8), tp=home)
    signal(tp=1 - c)
    for d in (1, 2, 3):
        signal(x=lax.rem(x + d, 4))
    signal(fs=lax.rem(y + 1, 4))
    signal(fs=lax.rem(y + 3, 4))
    first_x = x == 0
    heir = jnp.logical_and(first_x, z > 0)
    giver = z < 7

    @pl.when(heir)
    def _():
        for s in range(4):
            signal(z=z - 1, x=s)

    quarter = 2 * lax.rem(z, 2) + c
    head = 2 * x + lax.rem(z // 2, 2)
    wanted = x + lax.rem(z, 2) * (3 - 2 * x)
    for h in range(8):
        zh, xh, ch = 4 * c + 2 * (h % 2) + wanted // 2, h // 2, lax.rem(wanted, 2)
        self_ = jnp.logical_and(jnp.logical_and(zh == z, xh == x), ch == c)
        pl.when(other(self_))(lambda zh=zh, xh=xh, ch=ch: signal(z=zh, x=xh, tp=ch))
    backs = []
    mine = jnp.int32(0)
    for zq in range(NZ):
        xd = quarter if zq % 2 == 0 else 3 - quarter
        self_ = jnp.logical_and(jnp.logical_and(z == zq, xd == x), here)
        mine = mine + self_.astype(jnp.int32)
        copy = remote(oout.at[zq], oin.at[head], os_.at[zq], or_.at[head], z=zq, x=xd, tp=home)
        backs.append((self_, copy, zq))

    def norm(i, _):
        at = pl.ds(pl.multiple_of(i * 16, 16), 16)
        floats = tok[at, :].astype(F32)
        scale = lax.rsqrt(jnp.mean(floats * floats, axis=1, keepdims=True) + 1e-06)
        rows[x, c, at, :] = (floats * scale * tok_gain[...]).astype(BF16)
        return 0

    lax.fori_loop(0, 8, norm, 0)
    offs[x] = offx[x]
    for load in first_loads:
        load.wait()
    pl.semaphore_wait(
        pltpu.get_barrier_semaphore(),
        22 - here.astype(jnp.int32) + giver.astype(jnp.int32) - mine,
    )

    ring_w = Ring("fs", y, lambda b, h: weights.at[b, pl.ds(h * 256, 256)], cys, cyr)
    ring_x = Ring("x", x, lambda b, h: rows.at[b, c, pl.ds(h * 64, 64)], cxs, cxr)

    def over(block, slot):
        ref = rows.at[block, c]
        return remote(ref, ref, cds.at[slot], cdr.at[slot], tp=1 - c)

    across = [over(x, 0), over(ring_x.left, 1), over(ring_x.right, 2), over(lax.rem(x + 2, 4), 3)]
    ring_w.start()
    ring_x.start()
    across[0].start()
    small = [
        remote(offx.at[lax.rem(x + d, 4)], offs.at[x], cos.at[d - 1], cor.at[d - 1], x=lax.rem(x + d, 4))
        for d in (1, 2, 3)
    ]
    for copy in small:
        copy.start()
    lane = lax.broadcasted_iota(jnp.int32, (8, QB), 1)
    sub = lax.broadcasted_iota(jnp.int32, (8, QB), 0)

    def caps(i, _):
        key = sub * 128 + i
        rows = pl.ds(pl.multiple_of(i * 8, 8), 8)
        cap[0, rows, :] = jnp.full((8, QB), TOP, F32)
        cap[1, rows, :] = jnp.where(key < lane + quarter * QB, TOP, -300.0)
        cap[2, rows, :] = jnp.where(key < lane + (3 - quarter) * QB, TOP, -300.0)
        return 0

    lax.fori_loop(0, 128, caps, 0, unroll=4)
    ring_x.forward()
    ring_w.forward()
    ring_x.neighbours()
    across[1].start()
    across[2].start()
    ring_x.far()
    across[3].start()
    for copy in small:
        copy.wait()
    for load in loads:
        load.wait()
    for copy in across:
        copy.wait()
    ring_w.neighbours()

    def near(b, _):
        at = pl.ds(pl.multiple_of(b * 256, 256), 256)
        total = None
        for f in (y, ring_w.left, ring_w.right):
            cols = pl.ds(pl.multiple_of(f * 512, 512), 512)
            lhs = jnp.concatenate([rows[b, 0, :, cols], rows[b, 1, :, cols]], axis=0)
            part = jnp.dot(lhs, weights[f], preferred_element_type=F32)
            total = part if total is None else total + part
        full[at, :] = total
        return 0

    lax.fori_loop(0, 4, near, 0)
    ring_w.far()
    far = lax.rem(y + 2, 4)

    def block(b, _):
        at = pl.ds(pl.multiple_of(b * 256, 256), 256)
        cols = pl.ds(pl.multiple_of(far * 512, 512), 512)
        lhs = jnp.concatenate([rows[b, 0, :, cols], rows[b, 1, :, cols]], axis=0)
        total = full[at, :] + jnp.dot(lhs, weights[far], preferred_element_type=F32)
        kf[at, :] = total[:, 128:256]
        vf[at, :] = total[:, 256:384]
        q = total[:, :128].T
        qt[0, b] = q[:64].astype(BF16)
        qt[1, b] = q[64:].astype(BF16)
        value = total[:, 384:512].astype(BF16).astype(F32)
        gate = total[:, 512:640].astype(BF16).astype(F32)
        gated[at, :] = (value / (1.0 + jnp.exp(-gate))).astype(BF16)
        return 0

    lax.fori_loop(0, 4, block, 0)
    low = lax.broadcasted_iota(jnp.int32, (8, 128), 1) < 64

    def keys(i, _):
        packed = [[], []]
        for s in (0, 1):
            near_ = kf[pl.ds(2 * i + s, 8, stride=128), :]
            later = kf[pl.ds(2 * i + s + 64, 8, stride=128), :]
            packed[0].append(jnp.where(low, near_, pltpu.roll(later, 64, 1)))
            packed[1].append(jnp.where(low, pltpu.roll(near_, 64, 1), later))
        at = pl.ds(pl.multiple_of(i * 16, 16), 16)
        for j in (0, 1):
            kp[j, at, :] = jnp.concatenate(packed[j], axis=0).astype(BF16)
        return 0

    lax.fori_loop(0, 32, keys, 0, unroll=4)

    def ordered(i, _):
        vp[pl.ds(pl.multiple_of(i * 8, 8), 8), :] = vf[pl.ds(i, 8, stride=128), :]
        return 0

    lax.fori_loop(0, 128, ordered, 0, unroll=8)
    for b in range(8):
        v = vp[pl.ds(b * 128, 128), :].T.astype(BF16)
        vt[0, :, pl.ds(b * 128, 128)] = v[:64]
        vt[1, :, pl.ds(b * 128, 128)] = v[64:]
    sub_ = lax.broadcasted_iota(jnp.int32, (8, 128), 0)
    for j in (0, 1):
        tile = offs[0, j]
        for s in (1, 2, 3):
            tile = jnp.where(sub_ < 2 * s, tile, pltpu.roll(offs[s, j], 2 * s, 0))
        m[j] = tile

    sends = []

    def send(src, dst, slot, recv, zd, cd):
        same = jnp.logical_and(zd == z, cd == c)
        copy = remote(src, dst, zs.at[slot], recv, z=zd, tp=cd)
        pl.when(same)(local(src, dst, recv).start)
        pl.when(other(same))(copy.start)
        sends.append((other(same), copy))

    odd = lax.rem(z, 2)
    for e in range(4):
        jj = lax.rem(z + e, 4)
        zd, j, half = 4 * c + jj, jj // 2, lax.rem(jj, 2)
        for cd in (0, 1):
            q4 = 2 * half + cd
            send(qt.at[j, q4 + odd * (3 - 2 * q4)], qin.at[z], 6 * e + 2 + cd, qs.at[z], zd, cd)
            send(m.at[j], min_.at[z], 6 * e + 4 + cd, ms.at[z], zd, cd)
        send(kp.at[j], kin.at[z], 6 * e, ks.at[z], zd, 0)
        send(vt.at[j], vin.at[z], 6 * e + 1, vs.at[z], zd, 1)

    short = gated.at[pl.ds(0, 256), :]
    edge_rows = pl.ds(0, EDGE)

    def part(to):
        return gated.at[pl.ds(pl.multiple_of(to * 256 - EDGE, EDGE), 256 + EDGE), :]

    rows_x = []
    for d in (1, 2, 3):
        to = lax.rem(x + d, 4)
        whole = remote(part(to), gin.at[x], xs.at[d - 1], xr.at[x], x=to)
        less = remote(short, gin.at[x, pl.ds(EDGE, 256), :], xs.at[d - 1], xr.at[x], x=to)
        pl.when(to > 0)(whole.start)
        pl.when(to == 0)(less.start)
        rows_x.append((to, whole, less))
    pl.when(other(first_x))(local(part(x), gin.at[x], xr.at[x]).start)
    pl.when(first_x)(local(short, gin.at[x, pl.ds(EDGE, 256), :], xr.at[x]).start)
    edge = remote(
        gated.at[pl.ds(UNIT - EDGE, EDGE), :], gin.at[x, edge_rows, :], hs.at[0], hr.at[x], z=z + 1, x=0
    )
    pl.when(giver)(edge.start)
    ring_y = Ring("fs", y, lambda b, h: wout.at[b, h], ys, yr)
    ring_y.start()

    @pl.when(jnp.logical_and(first_x, z == 0))
    def _():
        for s in range(4):
            gin[s, edge_rows, :] = jnp.zeros((EDGE, 128), BF16)

    for s in range(4):
        pl.when(other(first_x))(local(part(1), gin.at[s], xr.at[s]).wait)
        pl.when(first_x)(local(short, gin.at[s, pl.ds(EDGE, 256), :], xr.at[s]).wait)
        pl.when(heir)(local(gated.at[edge_rows, :], gin.at[s, edge_rows, :], hr.at[s]).wait)
    for s in range(4):
        ext[s] = gin[s].astype(F32)
    for s in range(4):
        cols = pl.ds(s * 128, 128)

        def block(i, _, s=s, cols=cols):
            at = pl.multiple_of(i * 32, 32)
            total = jnp.zeros((32, 128), F32)
            for tap in range(KW):
                total = total + taps[pl.ds(tap, 1), cols] * ext[s, pl.ds(at + EDGE - (KW - 1) + tap, 32), :]
            rows = pl.ds(at, 32)
            csum[rows, cols] = total
            square = total * total
            if s > 0:
                total = total + stat[0, rows, :]
                square = square + stat[1, rows, :]
            if s == 3:
                total = jnp.broadcast_to(jnp.sum(total, axis=1, keepdims=True), (32, 128))
                square = jnp.broadcast_to(jnp.sum(square, axis=1, keepdims=True), (32, 128))
            stat[0, rows, :] = total
            stat[1, rows, :] = square
            return 0

        lax.fori_loop(0, 8, block, 0)

    zero = jnp.zeros((HD, QB), BF16)
    row = lax.broadcasted_iota(jnp.int32, (128, QB), 0)
    one_a, one_b = ((row == i).astype(F32).astype(BF16) for i in (0, 1))
    col = lax.broadcasted_iota(jnp.int32, (8, 128), 1)

    def pass_on(at, source):
        ref, sem = (kin, ks) if at == 0 else (vin, vs)
        return remote(ref.at[source], ref.at[source], ds.at[source], sem.at[source], tp=1 - at)

    def arrive(n):
        source = lax.rem(z + nth(n), 8)
        for core in (0, 1):
            @pl.when(c == core)
            def _(core=core):
                copy = pass_on(core, source)
                copy.wait_recv()
                copy.start()

        pl.when(n == 3)(ring_y.forward)
        local(qt.at[0, 0], qin.at[source], qs.at[source]).wait()
        local(m.at[0], min_.at[source], ms.at[source]).wait()
        q = (qin[source].astype(F32) * 0.125).astype(BF16)
        qa[source] = jnp.concatenate([q, zero, one_a], axis=0)
        qb[source] = jnp.concatenate([zero, q, one_b], axis=0)
        tile = min_[source]
        for i in range(32):
            both = []
            for k in (2 * i, 2 * i + 1):
                near = jnp.broadcast_to(tile[:, k : k + 1], (8, 128))
                later = jnp.broadcast_to(tile[:, k + 64 : k + 65], (8, 128))
                both.append(jnp.where(col == 0, near, jnp.where(col == 1, later, 0.0)))
            off[source, pl.ds(i * 16, 16), :] = jnp.concatenate(both, axis=0).astype(BF16)
        for core in (0, 1):
            pl.when(c == core)(lambda core=core: pass_on(1 - core, source).wait_recv())

    def where_is(u):
        one, two = lax.rem(z + nth(u[0]), 8), lax.rem(z + nth(u[1]), 8)
        return jnp.maximum(one, two), jnp.minimum(one, two)

    def following(u):
        n, k = u
        ends = k == n
        return (jnp.where(ends, n + 1, n), jnp.where(ends, 0, k + 1))

    def scores(u, s_ref):
        pl.when(jnp.logical_and(u[1] == 0, u[0] < NZ))(lambda: arrive(u[0]))
        zq, zk = where_is((jnp.minimum(u[0], NZ - 1), u[1]))
        lhs = jnp.concatenate([kin[zk], off[zk]], axis=1)
        s_ref[0:512, :] = jnp.dot(lhs, qa[zq], preferred_element_type=F32)
        s_ref[512:1024, :] = jnp.dot(lhs, qb[zq], preferred_element_type=F32)

    def weights(u, s_ref, w_ref):
        zq, zk = where_is(u)
        which = jnp.where(zq == zk, 1 + lax.rem(zq, 2), 0)
        weigh(s_ref, cap.at[which], r_ref, w_ref, left.at[zq * NZ + zk])

    def values(u, w_ref):
        zq, zk = where_is(u)
        acc[zq * NZ + zk] = jnp.dot(vin[zk], w_ref[...], preferred_element_type=F32)

    start = jnp.int32(0)
    w1[...] = jnp.zeros_like(w1)
    scores((start, start), s0)

    remote(stat, stat_in, ss.at[0], sr.at[0], tp=1 - c).start()

    def pair(_, state):
        before, now = state
        after = following(now)
        scores(after, s1)
        weights(now, s0, w0)
        values(before, w1)
        last = following(after)
        scores(last, s0)
        weights(after, s1, w1)
        values(now, w0)
        return (after, last)

    last, _ = lax.fori_loop(0, NZ * (NZ + 1) // 4, pair, ((start, start), (start, start)))
    values(last, w1)

    for zq in range(NZ):
        total = acc[zq * NZ + zq].reshape(8, 8, QB)
        rest = left[zq * NZ + zq]
        for zk in range(zq - 1, -1, -1):
            total = total + acc[zq * NZ + zk].reshape(8, 8, QB) * rest[None]
            if zk > 0:
                rest = rest * left[zq * NZ + zk]
        oout[zq] = total.reshape(HD, QB).astype(BF16)
    for self_, copy, zq in backs:
        pl.when(other(self_))(copy.start)
        pl.when(self_)(local(oout.at[zq], oin.at[head], or_.at[head]).start)

    remote(stat, stat_in, ss.at[0], sr.at[0], tp=1 - c).wait()

    def finish(i, _):
        rows = pl.ds(pl.multiple_of(i * 32, 32), 32)
        mean = (stat[0, rows, :] + stat_in[0, rows, :]) / CC
        spread = (stat[1, rows, :] + stat_in[1, rows, :]) / CC - mean * mean
        scale = lax.rsqrt(spread + 1e-06)
        for s in range(4):
            cols = pl.ds(s * 128, 128)
            h = (csum[rows, cols] - mean) * scale * gain[:, cols]
            hidden[rows, cols] = (h / (1.0 + jnp.exp(-h))).astype(BF16)
        return 0

    lax.fori_loop(0, 8, finish, 0)
    ring_y.neighbours()
    ring_y.far()
    for h in range(8):
        local(oout.at[0], oin.at[h], or_.at[h]).wait()
    heads[...] = oin[...].reshape(512, QB).astype(F32).T.astype(BF16)
    theirs = []
    for f in range(4):
        total = jnp.dot(heads[...], wout[f, 0], preferred_element_type=F32)
        total = (total + jnp.dot(hidden[...], wout[f, 1], preferred_element_type=F32)).astype(BF16)
        low, high = total[:128], total[128:]
        own_part[f] = jnp.where(c == 0, low, high)
        part_out[f] = jnp.where(c == 0, high, low)
        theirs.append(remote(part_out.at[f], part_in.at[f], ps.at[f], pr.at[f], tp=1 - c))
    for copy in theirs:
        copy.start()
    for f, copy in enumerate(theirs):
        copy.wait()
        total = own_part[f].astype(F32) + part_in[f].astype(F32)
        out_ref[:, pl.ds(f * 512, 512)] = total.astype(BF16)

    for cond, copy in sends:
        pl.when(cond)(copy.wait_send)
    for to, whole, less in rows_x:
        pl.when(to > 0)(whole.wait_send)
        pl.when(to == 0)(less.wait_send)
    pl.when(giver)(edge.wait_send)
    for self_, copy, zq in backs:
        pl.when(other(self_))(copy.wait_send)
    for core in (0, 1):
        @pl.when(c == core)
        def _(core=core):
            for source in range(NZ):
                pass_on(core, source).wait_send()

    ring_y.sent()
    ring_x.sent()
    ring_w.sent()


def layer(tokens, tok_gain, offx, taps, gain, *ws):
    vm = pltpu.VMEM
    return pl.pallas_call(
        layer_kernel,
        out_shape=jax.ShapeDtypeStruct((128, 2048), BF16),
        in_specs=[VM] * 5 + [HBM] * 7,
        out_specs=VM,
        scratch_shapes=[
            vm((NX, 2, 128, 2048), BF16),
            vm((4, 512, 640), BF16),
            vm((NX, 2, 8, 128), F32),
            vm((UNIT, 640), F32),
            vm((UNIT, 128), F32),
            vm((UNIT, 128), F32),
            vm((UNIT, 128), F32),
            vm((2, 4, HD, QB), BF16),
            vm((2, 512, 128), BF16),
            vm((2, HD, UNIT), BF16),
            vm((2, 8, 128), F32),
            vm((UNIT, 128), BF16),
            vm((NZ, 512, 128), BF16),
            vm((NZ, HD, UNIT), BF16),
            vm((NZ, HD, QB), BF16),
            vm((NZ, 8, 128), F32),
            vm((NX, 256 + EDGE, 128), BF16),
            vm((4, 2, 512, 512), BF16),
            vm((NX, 256 + EDGE, 128), F32),
            vm((256, 512), F32),
            vm((2, 256, 128), F32),
            vm((2, 256, 128), F32),
            vm((256, 512), BF16),
            vm((256, 512), BF16),
            vm((4, 128, 512), BF16),
            vm((4, 128, 512), BF16),
            vm((4, 128, 512), BF16),
            vm((NZ, 256, QB), BF16),
            vm((NZ, 256, QB), BF16),
            vm((NZ, 512, 128), BF16),
            vm((UNIT, QB), F32),
            vm((UNIT, QB), F32),
            vm((UNIT, QB), BF16),
            vm((UNIT, QB), BF16),
            vm((256, QB), F32),
            vm((3, UNIT, QB), F32),
            vm((NZ * NZ, 8, QB), F32),
            vm((NZ * NZ, HD, QB), F32),
            vm((NZ, HD, QB), BF16),
            vm((8, HD, QB), BF16),
        ]
        + sems(5, 6, 6, 6, 6, 4, 4, 3, 3)
        + sems(2, 6, 6, 24, 8, 8, 8, 8, 8, 8, 3, 4, 1, 4, 1, 1, 8, 8, 4, 4),
        compiler_params=pltpu.CompilerParams(
            collective_id=1, has_side_effects=True, vmem_limit_bytes=63 * 2**20
        ),
        name="layer",
    )(tokens, tok_gain, offx, taps, gain, *ws)


def shards(
    tokens, norm_gain, w_query, w_key, w_value, w_conv_value, w_conv_gate,
    key_offset, conv_kernel, conv_gain, w_attn_out, w_conv_out,
):
    tile = key_offset.astype(F32).T.reshape(NX, 2, 2, 128)
    tile = jnp.pad(tile, ((0, 0), (0, 0), (0, 6), (0, 0)))
    return layer(
        tokens[0], norm_gain[None], tile, conv_kernel, conv_gain[None],
        w_query, w_key, w_value, w_conv_value, w_conv_gate, w_attn_out, w_conv_out,
    )[None]


def solution(mesh):
    view = Mesh(mesh.devices.reshape(NZ, NX, 4, 2), ("z", "x", "fs", "tp"))
    rows = P("fs", ("z", "x", "tp"), None)
    placed = (
        rows, P(), P("fs", "tp"), P("fs", "tp"), P("fs", "tp"), P("fs", "tp"), P("fs", "tp"),
        P(("z", "x"), "tp"), P(None, "tp"), P("tp"), P("tp", "fs"), P("tp", "fs"),
    )
    return jax.shard_map(shards, mesh=view, in_specs=placed, out_specs=rows, check_vma=False)
```

```python
import functools
import math

import jax
import jax.numpy as jnp
from jax import lax
from jax.experimental import pallas as pl
from jax.experimental.pallas import tpu as pltpu
from jax.sharding import Mesh
from jax.sharding import PartitionSpec as P

MESH = pl.DeviceIdType.MESH
F32 = jnp.float32
BF16 = jnp.bfloat16
LOG2E = math.log2(math.e)
TOP = 25.0
HD = 64
CC = 1024
KW = 31
UNIT = 1024
QB = 256
NZ = 8
NX = 4
EDGE = 32
VM = pl.BlockSpec(memory_space=pltpu.VMEM)
HBM = pl.BlockSpec(memory_space=pltpu.HBM)


def sems(*counts):
    return [pltpu.SemaphoreType.DMA((n,)) for n in counts]


def remote(src, dst, send, recv, **to):
    return pltpu.make_async_remote_copy(
        src_ref=src, dst_ref=dst, send_sem=send, recv_sem=recv, device_id=to, device_id_type=MESH
    )


def signal(**to):
    pl.semaphore_signal(
        pltpu.get_barrier_semaphore(), inc=1, device_id=to, device_id_type=MESH
    )


class Ring:
    def __init__(self, axis, me, at, send, recv):
        right, left = lax.rem(me + 1, 4), lax.rem(me + 3, 4)
        self.left, self.right = left, right

        def hop(block, half, slot, to):
            ref = at(block, half)
            return remote(ref, ref, send.at[slot], recv.at[slot], **{axis: to})

        self.first = [hop(me, 0, 0, right), hop(me, 1, 2, left), hop(me, 1, 1, right), hop(me, 0, 3, left)]
        self.second = [hop(left, 0, 4, right), hop(right, 1, 5, left)]

    def start(self):
        for copy in self.first:
            copy.start()

    def forward(self):
        for got, copy in zip(self.first[:2], self.second):
            got.wait_recv()
            copy.start()

    def neighbours(self):
        for copy in self.first[2:]:
            copy.wait_recv()

    def far(self):
        for copy in self.second:
            copy.wait_recv()

    def sent(self):
        for copy in self.first + self.second:
            copy.wait_send()


def suffix(t):
    sub = lax.broadcasted_iota(jnp.int32, t.shape, 0)
    e = jnp.where(sub < 7, pltpu.roll(t, 7, 0), 1.0)
    for step in (1, 2, 4):
        e = e * jnp.where(sub < 8 - step, pltpu.roll(e, 8 - step, 0), 1.0)
    return e


def keep(score, cap, e_ref, r_ref, t_ref):
    t = None
    for g in [n // 2 + 16 * (n % 2) for n in range(32)]:
        d = []
        for j in range(4):
            i = 4 * g + j
            rows = pl.ds(i * 8, 8)
            e = jnp.exp2(jnp.minimum(score[i * 8 : i * 8 + 8], cap[rows, :]))
            e_ref[rows, :] = e
            d.append(e + 1.0)
        r = 1.0 / ((d[0] * d[1]) * (d[2] * d[3]))
        r_ref[pl.ds(g * 8, 8), :] = r
        t = r if t is None else t * r
    t_ref[...] = t


def weigh(e_ref, r_ref, t_ref, w_ref, left):
    t = t_ref[...]
    p = suffix(t)
    left[...] = jnp.broadcast_to((p * t)[0:1, :], p.shape)
    for g in range(31, -1, -1):
        p = p * r_ref[pl.ds(g * 8, 8), :]
        rest, w = p, []
        for j in range(4):
            w.append(e_ref[pl.ds((4 * g + j) * 8, 8), :] * rest)
            rest = rest + w[j]
        w_ref[pl.ds(g * 32, 32), :] = jnp.concatenate(w, axis=0).astype(BF16)


ARRIVAL = (0, 7, 3, 1, 5, 6, 2, 4)


def nth(n):
    d = jnp.int32(ARRIVAL[0])
    for k in range(1, NZ):
        d = jnp.where(n == k, ARRIVAL[k], d)
    return d


def layer_kernel(
    tok, tok_gain, offx, taps, gain, wq, wk, wv, wcv, wcg, wa, wc, out_ref,
    rows, weights, offs, full, kf, vf, vp, qt, kp, vt, m, gated,
    kin, vin, qin, min_, gin, wout, ext, csum, stat, stat_in, hidden, heads, own_part, part_out, part_in,
    qa, keys_in, e0, e1, w0, w1, r0, r1, t0, t1, cap, left, acc, oout, oin,
    ws, cxs, cxr, cys, cyr, cds, cdr, cos, cor,
    wl, ys, yr, zs, ks, vs, qs, ms, ds, fs, xs, xr, hs, hr, ss, sr, os_, or_, ps, pr,
):
    z, x, y, c = (lax.axis_index(n) for n in ("z", "x", "fs", "tp"))
    first_loads = [
        pltpu.make_async_copy(
            w.at[:, pl.ds(pl.multiple_of(x * 128, 128), 128)], weights.at[y, :, pl.ds(i * 128, 128)], ws.at[i]
        )
        for i, w in enumerate((wq, wk, wv, wcv, wcg))
    ]
    loads = [pltpu.make_async_copy(w, wout.at[y, i], wl.at[i]) for i, w in enumerate((wa, wc))]
    for load in first_loads + loads:
        load.start()
    home = z // 4
    here = home == c
    other = jnp.logical_not
    local = pltpu.make_async_copy
    for d in range(8):
        if d == 0:
            pl.when(other(here))(lambda: signal(tp=1 - c))
        else:
            signal(z=lax.rem(z + d, 8), tp=home)
    partner = z + 1 - 2 * lax.rem(z, 2)
    signal(tp=1 - c)
    signal(z=partner)
    for d in (1, 2, 3):
        signal(x=lax.rem(x + d, 4))
    signal(fs=lax.rem(y + 1, 4))
    signal(fs=lax.rem(y + 3, 4))
    first_x = x == 0
    heir = jnp.logical_and(first_x, z > 0)
    giver = z < 7

    @pl.when(heir)
    def _():
        for s in range(4):
            signal(z=z - 1, x=s)

    quarter = 2 * lax.rem(z, 2) + c
    head = 2 * x + lax.rem(z // 2, 2)
    wanted = x + lax.rem(z, 2) * (3 - 2 * x)
    for h in range(8):
        zh, xh, ch = 4 * c + 2 * (h % 2) + wanted // 2, h // 2, lax.rem(wanted, 2)
        self_ = jnp.logical_and(jnp.logical_and(zh == z, xh == x), ch == c)
        pl.when(other(self_))(lambda zh=zh, xh=xh, ch=ch: signal(z=zh, x=xh, tp=ch))
    backs = []
    mine = jnp.int32(0)
    for zq in range(NZ):
        xd = quarter if zq % 2 == 0 else 3 - quarter
        self_ = jnp.logical_and(jnp.logical_and(z == zq, xd == x), here)
        mine = mine + self_.astype(jnp.int32)
        copy = remote(oout.at[zq], oin.at[head], os_.at[zq], or_.at[head], z=zq, x=xd, tp=home)
        backs.append((self_, copy, zq))

    def norm(i, _):
        at = pl.ds(pl.multiple_of(i * 16, 16), 16)
        floats = tok[at, :].astype(F32)
        scale = lax.rsqrt(jnp.mean(floats * floats, axis=1, keepdims=True) + 1e-06)
        rows[x, c, at, :] = (floats * scale * tok_gain[...]).astype(BF16)
        return 0

    lax.fori_loop(0, 8, norm, 0)
    offs[x] = offx[x]
    for load in first_loads:
        load.wait()
    pl.semaphore_wait(
        pltpu.get_barrier_semaphore(),
        23 - here.astype(jnp.int32) + giver.astype(jnp.int32) - mine,
    )

    ring_w = Ring("fs", y, lambda b, h: weights.at[b, pl.ds(h * 256, 256)], cys, cyr)
    ring_x = Ring("x", x, lambda b, h: rows.at[b, c, pl.ds(h * 64, 64)], cxs, cxr)

    def over(block, slot):
        ref = rows.at[block, c]
        return remote(ref, ref, cds.at[slot], cdr.at[slot], tp=1 - c)

    across = [over(x, 0), over(ring_x.left, 1), over(ring_x.right, 2), over(lax.rem(x + 2, 4), 3)]
    ring_w.start()
    ring_x.start()
    across[0].start()
    small = [
        remote(offx.at[lax.rem(x + d, 4)], offs.at[x], cos.at[d - 1], cor.at[d - 1], x=lax.rem(x + d, 4))
        for d in (1, 2, 3)
    ]
    for copy in small:
        copy.start()
    lane = lax.broadcasted_iota(jnp.int32, (8, QB), 1)
    sub = lax.broadcasted_iota(jnp.int32, (8, QB), 0)

    def caps(i, _):
        key = sub * 128 + i
        rows = pl.ds(pl.multiple_of(i * 8, 8), 8)
        cap[0, rows, :] = jnp.full((8, QB), TOP, F32)
        cap[1, rows, :] = jnp.where(key < lane + quarter * QB, TOP, -300.0)
        cap[2, rows, :] = jnp.where(key < lane + (3 - quarter) * QB, TOP, -300.0)
        return 0

    lax.fori_loop(0, 128, caps, 0, unroll=4)
    ring_x.forward()
    ring_w.forward()
    ring_x.neighbours()
    across[1].start()
    across[2].start()
    for load in loads:
        load.wait()
    ring_w.neighbours()

    def near(b):
        at = pl.ds(pl.multiple_of(b * 256, 256), 256)
        total = None
        for f in (y, ring_w.left, ring_w.right):
            cols = pl.ds(pl.multiple_of(f * 512, 512), 512)
            lhs = jnp.concatenate([rows[b, 0, :, cols], rows[b, 1, :, cols]], axis=0)
            part = jnp.dot(lhs, weights[f], preferred_element_type=F32)
            total = part if total is None else total + part
        full[at, :] = total

    across[0].wait()
    near(x)
    across[1].wait()
    near(ring_x.left)
    ring_x.far()
    across[3].start()
    across[2].wait()
    near(ring_x.right)
    for copy in small:
        copy.wait()
    across[3].wait()
    near(lax.rem(x + 2, 4))
    ring_w.far()
    far = lax.rem(y + 2, 4)

    def block(b, _):
        at = pl.ds(pl.multiple_of(b * 256, 256), 256)
        cols = pl.ds(pl.multiple_of(far * 512, 512), 512)
        lhs = jnp.concatenate([rows[b, 0, :, cols], rows[b, 1, :, cols]], axis=0)
        total = full[at, :] + jnp.dot(lhs, weights[far], preferred_element_type=F32)
        kf[at, :] = total[:, 128:256]
        vf[at, :] = total[:, 256:384]
        q = total[:, :128].T
        qt[0, b] = q[:64].astype(BF16)
        qt[1, b] = q[64:].astype(BF16)
        value = total[:, 384:512].astype(BF16).astype(F32)
        gate = total[:, 512:640].astype(BF16).astype(F32)
        gated[at, :] = (value / (1.0 + jnp.exp(-gate))).astype(BF16)
        return 0

    lax.fori_loop(0, 4, block, 0)
    low = lax.broadcasted_iota(jnp.int32, (8, 128), 1) < 64

    def keys(i, _):
        packed = [[], []]
        for s in (0, 1):
            near_ = kf[pl.ds(2 * i + s, 8, stride=128), :]
            later = kf[pl.ds(2 * i + s + 64, 8, stride=128), :]
            packed[0].append(jnp.where(low, near_, pltpu.roll(later, 64, 1)))
            packed[1].append(jnp.where(low, pltpu.roll(near_, 64, 1), later))
        at = pl.ds(pl.multiple_of(i * 16, 16), 16)
        for j in (0, 1):
            kp[j, at, :] = jnp.concatenate(packed[j], axis=0).astype(BF16)
        return 0

    lax.fori_loop(0, 32, keys, 0, unroll=4)

    def ordered(i, _):
        vp[pl.ds(pl.multiple_of(i * 8, 8), 8), :] = vf[pl.ds(i, 8, stride=128), :]
        return 0

    lax.fori_loop(0, 128, ordered, 0, unroll=8)
    for b in range(8):
        v = vp[pl.ds(b * 128, 128), :].T.astype(BF16)
        vt[0, :, pl.ds(b * 128, 128)] = v[:64]
        vt[1, :, pl.ds(b * 128, 128)] = v[64:]
    sub_ = lax.broadcasted_iota(jnp.int32, (8, 128), 0)
    for j in (0, 1):
        tile = offs[0, j]
        for s in (1, 2, 3):
            tile = jnp.where(sub_ < 2 * s, tile, pltpu.roll(offs[s, j], 2 * s, 0))
        m[j] = tile

    sends = []

    def send(src, dst, slot, recv, zd, cd, cond=None):
        same = jnp.logical_and(zd == z, cd == c)
        away = other(same) if cond is None else jnp.logical_and(other(same), cond)
        near_ = same if cond is None else jnp.logical_and(same, cond)
        copy = remote(src, dst, zs.at[slot], recv, z=zd, tp=cd)
        pl.when(near_)(local(src, dst, recv).start)
        pl.when(away)(copy.start)
        sends.append((away, copy))

    odd = lax.rem(z, 2)
    short = gated.at[pl.ds(0, 256), :]
    edge_rows = pl.ds(0, EDGE)

    def part(to):
        return gated.at[pl.ds(pl.multiple_of(to * 256 - EDGE, EDGE), 256 + EDGE), :]

    rows_x = []
    for d in (1, 2, 3):
        to = lax.rem(x + d, 4)
        whole = remote(part(to), gin.at[x], xs.at[d - 1], xr.at[x], x=to)
        less = remote(short, gin.at[x, pl.ds(EDGE, 256), :], xs.at[d - 1], xr.at[x], x=to)
        pl.when(to > 0)(whole.start)
        pl.when(to == 0)(less.start)
        rows_x.append((to, whole, less))
    pl.when(other(first_x))(local(part(x), gin.at[x], xr.at[x]).start)
    pl.when(first_x)(local(short, gin.at[x, pl.ds(EDGE, 256), :], xr.at[x]).start)
    edge = remote(
        gated.at[pl.ds(UNIT - EDGE, EDGE), :], gin.at[x, edge_rows, :], hs.at[0], hr.at[x], z=z + 1, x=0
    )
    pl.when(giver)(edge.start)
    for e in (0, 1, 3, 2):
        jj = lax.rem(z + e, 4)
        zd, j, half = 4 * c + jj, jj // 2, lax.rem(jj, 2)
        for cd in (0, 1):
            q4 = 2 * half + cd
            send(qt.at[j, q4 + odd * (3 - 2 * q4)], qin.at[z], 6 * e + 2 + cd, qs.at[z], zd, cd)
            send(m.at[j], min_.at[z], 6 * e + 4 + cd, ms.at[z], zd, cd)
        send(kp.at[j], kin.at[z], 6 * e, ks.at[z], zd, 0, here if e == 0 else None)
        send(vt.at[j], vin.at[z], 6 * e + 1, vs.at[z], zd, 1, here if e == 0 else None)
    ring_y = Ring("fs", y, lambda b, h: wout.at[b, h], ys, yr)
    ring_y.start()

    @pl.when(jnp.logical_and(first_x, z == 0))
    def _():
        for s in range(4):
            gin[s, edge_rows, :] = jnp.zeros((EDGE, 128), BF16)

    for s in range(4):
        pl.when(other(first_x))(local(part(1), gin.at[s], xr.at[s]).wait)
        pl.when(first_x)(local(short, gin.at[s, pl.ds(EDGE, 256), :], xr.at[s]).wait)
        pl.when(heir)(local(gated.at[edge_rows, :], gin.at[s, edge_rows, :], hr.at[s]).wait)
    for s in range(4):
        ext[s] = gin[s].astype(F32)
    for s in range(4):
        cols = pl.ds(s * 128, 128)

        def block(i, _, s=s, cols=cols):
            at = pl.multiple_of(i * 32, 32)
            total = jnp.zeros((32, 128), F32)
            for tap in range(KW):
                total = total + taps[pl.ds(tap, 1), cols] * ext[s, pl.ds(at + EDGE - (KW - 1) + tap, 32), :]
            rows = pl.ds(at, 32)
            csum[rows, cols] = total
            square = total * total
            if s > 0:
                total = total + stat[0, rows, :]
                square = square + stat[1, rows, :]
            if s == 3:
                total = jnp.broadcast_to(jnp.sum(total, axis=1, keepdims=True), (32, 128))
                square = jnp.broadcast_to(jnp.sum(square, axis=1, keepdims=True), (32, 128))
            stat[0, rows, :] = total
            stat[1, rows, :] = square
            return 0

        lax.fori_loop(0, 8, block, 0)

    zero = jnp.zeros((HD, QB), BF16)
    ones = (lax.broadcasted_iota(jnp.int32, (HD, QB), 0) < 2).astype(F32).astype(BF16)
    col = lax.broadcasted_iota(jnp.int32, (8, 128), 1)

    def pass_on(at, source):
        ref, sem = (kin, ks) if at == 0 else (vin, vs)
        return remote(ref.at[source], ref.at[source], ds.at[source], sem.at[source], tp=1 - at)

    opposite = lax.rem(partner + 4, 8)

    def hand_on(at):
        ref, sem = (kin, ks) if at == 0 else (vin, vs)
        return remote(ref.at[opposite], ref.at[opposite], fs.at[0], sem.at[opposite], z=partner)

    def share(n):
        source = lax.rem(z + nth(n), 8)
        for core in (0, 1):
            @pl.when(c == core)
            def _(core=core):
                copy = pass_on(core, source)
                copy.wait_recv()
                pl.when(source == opposite)(hand_on(core).start)
                copy.start()

    def arrive(n):
        source = lax.rem(z + nth(n), 8)
        pl.when(n < NZ - 1)(lambda: share(n + 1))
        pl.when(n == 3)(ring_y.forward)
        local(qt.at[0, 0], qin.at[source], qs.at[source]).wait()
        local(m.at[0], min_.at[source], ms.at[source]).wait()
        q = qin[source].astype(F32) * (HD**-0.5 * LOG2E)
        high = q.astype(BF16)
        qa[source] = jnp.concatenate([high, ones, (q - high.astype(F32)).astype(BF16), zero], axis=0)
        for core in (0, 1):
            pl.when(c == core)(lambda core=core: pass_on(1 - core, source).wait_recv())
        tile = min_[source] * LOG2E
        for i in range(32):
            packed = kin[source, pl.ds(i * 16, 16), :].astype(F32)
            for first in (0, 64):
                both = []
                for k in (0, 1):
                    at = first + 2 * i + k
                    value = jnp.broadcast_to(tile[:, at : at + 1], (8, 128))
                    top = value.astype(BF16).astype(F32)
                    key = packed[8 * k : 8 * k + 8]
                    key = pltpu.roll(key, 64, 1) if first else key
                    extra = jnp.where(col == HD, top, jnp.where(col == HD + 1, value - top, 0.0))
                    both.append(jnp.where(col < HD, key, extra))
                keys_in[source, pl.ds(first * 8 + i * 16, 16), :] = jnp.concatenate(both, axis=0).astype(BF16)

    def where_is(u):
        one, two = lax.rem(z + nth(u[0]), 8), lax.rem(z + nth(u[1]), 8)
        return jnp.maximum(one, two), jnp.minimum(one, two)

    def following(u):
        n, k = u
        ends = k == n
        return (jnp.where(ends, n + 1, n), jnp.where(ends, 0, k + 1))

    def ready(u):
        pl.when(jnp.logical_and(u[1] == 0, u[0] < NZ))(lambda: arrive(u[0]))

    def scores(u, e_ref, r_ref, t_ref):
        zq, zk = where_is((jnp.minimum(u[0], NZ - 1), u[1]))
        keys_ = keys_in[zk]
        score = jnp.dot(jnp.concatenate([keys_, keys_], axis=1), qa[zq], preferred_element_type=F32)
        which = jnp.where(zq == zk, 1 + lax.rem(zq, 2), 0)
        keep(score, cap.at[which], e_ref, r_ref, t_ref)

    def weights_of(u, e_ref, r_ref, t_ref, w_ref):
        zq, zk = where_is(u)
        weigh(e_ref, r_ref, t_ref, w_ref, left.at[zq * NZ + zk])

    def values(u, w_ref):
        zq, zk = where_is(u)
        acc[zq * NZ + zk] = jnp.dot(vin[zk], w_ref[...], preferred_element_type=F32)

    start = jnp.int32(0)
    w1[...] = jnp.zeros_like(w1)
    share(start)
    ready((start, start))
    scores((start, start), e0, r0, t0)
    remote(stat, stat_in, ss.at[0], sr.at[0], tp=1 - c).start()

    def pair(_, state):
        before, now = state
        after = following(now)
        last = following(after)
        ready(after)
        ready(last)
        scores(after, e1, r1, t1)
        weights_of(now, e0, r0, t0, w0)
        values(before, w1)
        scores(last, e0, r0, t0)
        weights_of(after, e1, r1, t1, w1)
        values(now, w0)
        return (after, last)

    last, _ = lax.fori_loop(0, NZ * (NZ + 1) // 4, pair, ((start, start), (start, start)))
    values(last, w1)

    for zq in range(NZ):
        total = acc[zq * NZ + zq].reshape(8, 8, QB)
        rest = left[zq * NZ + zq]
        for zk in range(zq - 1, -1, -1):
            total = total + acc[zq * NZ + zk].reshape(8, 8, QB) * rest[None]
            if zk > 0:
                rest = rest * left[zq * NZ + zk]
        oout[zq] = total.reshape(HD, QB).astype(BF16)
    for self_, copy, zq in backs:
        pl.when(other(self_))(copy.start)
        pl.when(self_)(local(oout.at[zq], oin.at[head], or_.at[head]).start)

    remote(stat, stat_in, ss.at[0], sr.at[0], tp=1 - c).wait()

    def finish(i, _):
        rows = pl.ds(pl.multiple_of(i * 32, 32), 32)
        mean = (stat[0, rows, :] + stat_in[0, rows, :]) / CC
        spread = (stat[1, rows, :] + stat_in[1, rows, :]) / CC - mean * mean
        scale = lax.rsqrt(spread + 1e-06)
        for s in range(4):
            cols = pl.ds(s * 128, 128)
            h = (csum[rows, cols] - mean) * scale * gain[:, cols]
            hidden[rows, cols] = (h / (1.0 + jnp.exp(-h))).astype(BF16)
        return 0

    lax.fori_loop(0, 8, finish, 0)
    ring_y.neighbours()
    ring_y.far()
    for h in range(8):
        local(oout.at[0], oin.at[h], or_.at[h]).wait()
    heads[...] = oin[...].reshape(512, QB).astype(F32).T.astype(BF16)
    theirs = []
    for f in range(4):
        total = jnp.dot(heads[...], wout[f, 0], preferred_element_type=F32)
        total = (total + jnp.dot(hidden[...], wout[f, 1], preferred_element_type=F32)).astype(BF16)
        low, high = total[:128], total[128:]
        own_part[f] = jnp.where(c == 0, low, high)
        part_out[f] = jnp.where(c == 0, high, low)
        theirs.append(remote(part_out.at[f], part_in.at[f], ps.at[f], pr.at[f], tp=1 - c))
        if f > 0:
            theirs[f - 1].start()
    theirs[3].start()
    for f, copy in enumerate(theirs):
        copy.wait()
        total = own_part[f].astype(F32) + part_in[f].astype(F32)
        out_ref[:, pl.ds(f * 512, 512)] = total.astype(BF16)

    for cond, copy in sends:
        pl.when(cond)(copy.wait_send)
    for to, whole, less in rows_x:
        pl.when(to > 0)(whole.wait_send)
        pl.when(to == 0)(less.wait_send)
    pl.when(giver)(edge.wait_send)
    for self_, copy, zq in backs:
        pl.when(other(self_))(copy.wait_send)
    for core in (0, 1):
        @pl.when(c == core)
        def _(core=core):
            for source in range(NZ):
                pass_on(core, source).wait_send()
            hand_on(core).wait_send()

    ring_y.sent()
    ring_x.sent()
    ring_w.sent()


def layer(tokens, tok_gain, offx, taps, gain, *ws):
    vm = pltpu.VMEM
    return pl.pallas_call(
        layer_kernel,
        out_shape=jax.ShapeDtypeStruct((128, 2048), BF16),
        in_specs=[VM] * 5 + [HBM] * 7,
        out_specs=VM,
        scratch_shapes=[
            vm((NX, 2, 128, 2048), BF16),
            vm((4, 512, 640), BF16),
            vm((NX, 2, 8, 128), F32),
            vm((UNIT, 640), F32),
            vm((UNIT, 128), F32),
            vm((UNIT, 128), F32),
            vm((UNIT, 128), F32),
            vm((2, 4, HD, QB), BF16),
            vm((2, 512, 128), BF16),
            vm((2, HD, UNIT), BF16),
            vm((2, 8, 128), F32),
            vm((UNIT, 128), BF16),
            vm((NZ, 512, 128), BF16),
            vm((NZ, HD, UNIT), BF16),
            vm((NZ, HD, QB), BF16),
            vm((NZ, 8, 128), F32),
            vm((NX, 256 + EDGE, 128), BF16),
            vm((4, 2, 512, 512), BF16),
            vm((NX, 256 + EDGE, 128), F32),
            vm((256, 512), F32),
            vm((2, 256, 128), F32),
            vm((2, 256, 128), F32),
            vm((256, 512), BF16),
            vm((256, 512), BF16),
            vm((4, 128, 512), BF16),
            vm((4, 128, 512), BF16),
            vm((4, 128, 512), BF16),
            vm((NZ, 256, QB), BF16),
            vm((NZ, UNIT, 128), BF16),
            vm((UNIT, QB), F32),
            vm((UNIT, QB), F32),
            vm((UNIT, QB), BF16),
            vm((UNIT, QB), BF16),
            vm((256, QB), F32),
            vm((256, QB), F32),
            vm((8, QB), F32),
            vm((8, QB), F32),
            vm((3, UNIT, QB), F32),
            vm((NZ * NZ, 8, QB), F32),
            vm((NZ * NZ, HD, QB), F32),
            vm((NZ, HD, QB), BF16),
            vm((8, HD, QB), BF16),
        ]
        + sems(5, 6, 6, 6, 6, 4, 4, 3, 3)
        + sems(2, 6, 6, 24, 8, 8, 8, 8, 8, 1, 3, 4, 1, 4, 1, 1, 8, 8, 4, 4),
        compiler_params=pltpu.CompilerParams(
            collective_id=1, has_side_effects=True, vmem_limit_bytes=63 * 2**20
        ),
        name="layer",
    )(tokens, tok_gain, offx, taps, gain, *ws)


def shards(
    tokens, norm_gain, w_query, w_key, w_value, w_conv_value, w_conv_gate,
    key_offset, conv_kernel, conv_gain, w_attn_out, w_conv_out,
):
    tile = key_offset.astype(F32).T.reshape(NX, 2, 2, 128)
    tile = jnp.pad(tile, ((0, 0), (0, 0), (0, 6), (0, 0)))
    return layer(
        tokens[0], norm_gain[None], tile, conv_kernel, conv_gain[None],
        w_query, w_key, w_value, w_conv_value, w_conv_gate, w_attn_out, w_conv_out,
    )[None]


def solution(mesh):
    view = Mesh(mesh.devices.reshape(NZ, NX, 4, 2), ("z", "x", "fs", "tp"))
    rows = P("fs", ("z", "x", "tp"), None)
    placed = (
        rows, P(), P("fs", "tp"), P("fs", "tp"), P("fs", "tp"), P("fs", "tp"), P("fs", "tp"),
        P(("z", "x"), "tp"), P(None, "tp"), P("tp"), P("tp", "fs"), P("tp", "fs"),
    )
    return jax.shard_map(shards, mesh=view, in_specs=placed, out_specs=rows, check_vma=False)
```

```python
import functools
import math

import jax
import jax.numpy as jnp
from jax import lax
from jax.experimental import pallas as pl
from jax.experimental.pallas import tpu as pltpu
from jax.sharding import Mesh
from jax.sharding import PartitionSpec as P

MESH = pl.DeviceIdType.MESH
F32 = jnp.float32
BF16 = jnp.bfloat16
LOG2E = math.log2(math.e)
TOP = 25.0
HD = 64
CC = 1024
KW = 31
UNIT = 1024
QB = 256
NZ = 8
NX = 4
EDGE = 32
VM = pl.BlockSpec(memory_space=pltpu.VMEM)
HBM = pl.BlockSpec(memory_space=pltpu.HBM)


def sems(*counts):
    return [pltpu.SemaphoreType.DMA((n,)) for n in counts]


def remote(src, dst, send, recv, **to):
    return pltpu.make_async_remote_copy(
        src_ref=src, dst_ref=dst, send_sem=send, recv_sem=recv, device_id=to, device_id_type=MESH
    )


def signal(**to):
    pl.semaphore_signal(
        pltpu.get_barrier_semaphore(), inc=1, device_id=to, device_id_type=MESH
    )


class Ring:
    def __init__(self, axis, me, at, send, recv):
        right, left = lax.rem(me + 1, 4), lax.rem(me + 3, 4)
        self.left, self.right = left, right

        def hop(block, half, slot, to):
            ref = at(block, half)
            return remote(ref, ref, send.at[slot], recv.at[slot], **{axis: to})

        self.first = [hop(me, 0, 0, right), hop(me, 1, 2, left), hop(me, 1, 1, right), hop(me, 0, 3, left)]
        self.second = [hop(left, 0, 4, right), hop(right, 1, 5, left)]

    def start(self):
        for copy in self.first:
            copy.start()

    def forward(self):
        for got, copy in zip(self.first[:2], self.second):
            got.wait_recv()
            copy.start()

    def neighbours(self):
        for copy in self.first[2:]:
            copy.wait_recv()

    def far(self):
        for copy in self.second:
            copy.wait_recv()

    def sent(self):
        for copy in self.first + self.second:
            copy.wait_send()


def suffix(t):
    sub = lax.broadcasted_iota(jnp.int32, t.shape, 0)
    e = jnp.where(sub < 7, pltpu.roll(t, 7, 0), 1.0)
    for step in (1, 2, 4):
        e = e * jnp.where(sub < 8 - step, pltpu.roll(e, 8 - step, 0), 1.0)
    return e


def keep(score, cap, e_ref, r_ref, t_ref):
    t = None
    for g in [n // 2 + 16 * (n % 2) for n in range(32)]:
        d = []
        for j in range(4):
            i = 4 * g + j
            rows = pl.ds(i * 8, 8)
            e = jnp.exp2(jnp.minimum(score[i * 8 : i * 8 + 8], cap[rows, :]))
            e_ref[rows, :] = e
            d.append(e + 1.0)
        r = 1.0 / ((d[0] * d[1]) * (d[2] * d[3]))
        r_ref[pl.ds(g * 8, 8), :] = r
        t = r if t is None else t * r
    t_ref[...] = t


def weigh(e_ref, r_ref, t_ref, w_ref, left):
    t = t_ref[...]
    p = suffix(t)
    left[...] = jnp.broadcast_to((p * t)[0:1, :], p.shape)
    for g in range(31, -1, -1):
        p = p * r_ref[pl.ds(g * 8, 8), :]
        rest, w = p, []
        for j in range(4):
            w.append(e_ref[pl.ds((4 * g + j) * 8, 8), :] * rest)
            rest = rest + w[j]
        w_ref[pl.ds(g * 32, 32), :] = jnp.concatenate(w, axis=0).astype(BF16)


ARRIVAL = (0, 7, 3, 1, 5, 6, 2, 4)


def nth(n):
    d = jnp.int32(ARRIVAL[0])
    for k in range(1, NZ):
        d = jnp.where(n == k, ARRIVAL[k], d)
    return d


def layer_kernel(
    tok, tok_gain, offx, taps, gain, wq, wk, wv, wcv, wcg, wa, wc, own_part, part_in,
    rows, weights, offs, full, kf, vf, vp, qt, kp, vt, m, gated,
    kin, vin, qin, min_, gin, wout, ext, csum, stat, stat_in, hidden, heads, own_out, part_out, conv_part,
    qa, keys_in, e0, e1, w0, w1, r0, r1, t0, t1, cap, left, acc, oout, oin,
    ws, cxs, cxr, cys, cyr, cds, cdr, cos, cor,
    wl, ys, yr, zs, ks, vs, qs, ms, ds, fs, xs, xr, hs, hr, ss, sr, os_, or_, ps, pr, po,
):
    z, x, y, c = (lax.axis_index(n) for n in ("z", "x", "fs", "tp"))
    first_loads = [
        pltpu.make_async_copy(
            w.at[:, pl.ds(pl.multiple_of(x * 128, 128), 128)], weights.at[y, :, pl.ds(i * 128, 128)], ws.at[i]
        )
        for i, w in enumerate((wq, wk, wv, wcv, wcg))
    ]
    loads = [pltpu.make_async_copy(w, wout.at[y, i], wl.at[i]) for i, w in enumerate((wa, wc))]
    for load in first_loads + loads:
        load.start()
    home = z // 4
    here = home == c
    other = jnp.logical_not
    local = pltpu.make_async_copy
    for d in range(8):
        if d == 0:
            pl.when(other(here))(lambda: signal(tp=1 - c))
        else:
            signal(z=lax.rem(z + d, 8), tp=home)
    partner = z + 1 - 2 * lax.rem(z, 2)
    signal(tp=1 - c)
    signal(z=partner)
    for d in (1, 2, 3):
        signal(x=lax.rem(x + d, 4))
    signal(fs=lax.rem(y + 1, 4))
    signal(fs=lax.rem(y + 3, 4))
    first_x = x == 0
    heir = jnp.logical_and(first_x, z > 0)
    giver = z < 7

    @pl.when(heir)
    def _():
        for s in range(4):
            signal(z=z - 1, x=s)

    quarter = 2 * lax.rem(z, 2) + c
    head = 2 * x + lax.rem(z // 2, 2)
    wanted = x + lax.rem(z, 2) * (3 - 2 * x)
    for h in range(8):
        zh, xh, ch = 4 * c + 2 * (h % 2) + wanted // 2, h // 2, lax.rem(wanted, 2)
        self_ = jnp.logical_and(jnp.logical_and(zh == z, xh == x), ch == c)
        pl.when(other(self_))(lambda zh=zh, xh=xh, ch=ch: signal(z=zh, x=xh, tp=ch))
    backs = []
    mine = jnp.int32(0)
    for zq in range(NZ):
        xd = quarter if zq % 2 == 0 else 3 - quarter
        self_ = jnp.logical_and(jnp.logical_and(z == zq, xd == x), here)
        mine = mine + self_.astype(jnp.int32)
        copy = remote(oout.at[zq], oin.at[head], os_.at[zq], or_.at[head], z=zq, x=xd, tp=home)
        backs.append((self_, copy, zq))

    def norm(i, _):
        at = pl.ds(pl.multiple_of(i * 16, 16), 16)
        floats = tok[at, :].astype(F32)
        scale = lax.rsqrt(jnp.mean(floats * floats, axis=1, keepdims=True) + 1e-06)
        rows[x, c, at, :] = (floats * scale * tok_gain[...]).astype(BF16)
        return 0

    for load in first_loads:
        load.wait()
    pl.semaphore_wait(
        pltpu.get_barrier_semaphore(),
        23 - here.astype(jnp.int32) + giver.astype(jnp.int32) - mine,
    )

    ring_w = Ring("fs", y, lambda b, h: weights.at[b, pl.ds(h * 256, 256)], cys, cyr)
    ring_x = Ring("x", x, lambda b, h: rows.at[b, c, pl.ds(h * 64, 64)], cxs, cxr)

    def over(block, slot):
        ref = rows.at[block, c]
        return remote(ref, ref, cds.at[slot], cdr.at[slot], tp=1 - c)

    across = [over(x, 0), over(ring_x.left, 1), over(ring_x.right, 2), over(lax.rem(x + 2, 4), 3)]
    ring_w.start()
    lax.fori_loop(0, 8, norm, 0, unroll=4)
    offs[x] = offx[x]
    ring_x.start()
    across[0].start()
    small = [
        remote(offx.at[lax.rem(x + d, 4)], offs.at[x], cos.at[d - 1], cor.at[d - 1], x=lax.rem(x + d, 4))
        for d in (1, 2, 3)
    ]
    for copy in small:
        copy.start()
    lane = lax.broadcasted_iota(jnp.int32, (8, QB), 1)
    sub = lax.broadcasted_iota(jnp.int32, (8, QB), 0)

    def caps(i, _):
        key = sub * 128 + i
        rows = pl.ds(pl.multiple_of(i * 8, 8), 8)
        cap[0, rows, :] = jnp.full((8, QB), TOP, F32)
        cap[1, rows, :] = jnp.where(key < lane + quarter * QB, TOP, -300.0)
        cap[2, rows, :] = jnp.where(key < lane + (3 - quarter) * QB, TOP, -300.0)
        return 0

    lax.fori_loop(0, 128, caps, 0, unroll=4)
    ring_x.forward()
    ring_w.forward()
    ring_x.neighbours()
    across[1].start()
    across[2].start()
    for load in loads:
        load.wait()
    ring_w.neighbours()

    def near(b):
        at = pl.ds(pl.multiple_of(b * 256, 256), 256)
        total = None
        for f in (y, ring_w.left, ring_w.right):
            cols = pl.ds(pl.multiple_of(f * 512, 512), 512)
            lhs = jnp.concatenate([rows[b, 0, :, cols], rows[b, 1, :, cols]], axis=0)
            part = jnp.dot(lhs, weights[f], preferred_element_type=F32)
            total = part if total is None else total + part
        full[at, :] = total

    across[0].wait()
    near(x)
    across[1].wait()
    near(ring_x.left)
    ring_x.far()
    across[3].start()
    across[2].wait()
    near(ring_x.right)
    for copy in small:
        copy.wait()
    across[3].wait()
    near(lax.rem(x + 2, 4))
    ring_w.far()
    far = lax.rem(y + 2, 4)

    def block(b, _):
        at = pl.ds(pl.multiple_of(b * 256, 256), 256)
        cols = pl.ds(pl.multiple_of(far * 512, 512), 512)
        lhs = jnp.concatenate([rows[b, 0, :, cols], rows[b, 1, :, cols]], axis=0)
        total = full[at, :] + jnp.dot(lhs, weights[far], preferred_element_type=F32)
        kf[at, :] = total[:, 128:256]
        vf[at, :] = total[:, 256:384]
        q = total[:, :128].T
        qt[0, b] = q[:64].astype(BF16)
        qt[1, b] = q[64:].astype(BF16)
        value = total[:, 384:512].astype(BF16).astype(F32)
        gate = total[:, 512:640].astype(BF16).astype(F32)
        gated[at, :] = (value / (1.0 + jnp.exp(-gate))).astype(BF16)
        return 0

    lax.fori_loop(0, 4, block, 0)
    low = lax.broadcasted_iota(jnp.int32, (8, 128), 1) < 64

    def keys(i, _):
        packed = [[], []]
        for s in (0, 1):
            near_ = kf[pl.ds(2 * i + s, 8, stride=128), :]
            later = kf[pl.ds(2 * i + s + 64, 8, stride=128), :]
            packed[0].append(jnp.where(low, near_, pltpu.roll(later, 64, 1)))
            packed[1].append(jnp.where(low, pltpu.roll(near_, 64, 1), later))
        at = pl.ds(pl.multiple_of(i * 16, 16), 16)
        for j in (0, 1):
            kp[j, at, :] = jnp.concatenate(packed[j], axis=0).astype(BF16)
        return 0

    lax.fori_loop(0, 32, keys, 0, unroll=4)

    def ordered(i, _):
        vp[pl.ds(pl.multiple_of(i * 8, 8), 8), :] = vf[pl.ds(i, 8, stride=128), :]
        return 0

    lax.fori_loop(0, 128, ordered, 0, unroll=8)
    for b in range(8):
        v = vp[pl.ds(b * 128, 128), :].T.astype(BF16)
        vt[0, :, pl.ds(b * 128, 128)] = v[:64]
        vt[1, :, pl.ds(b * 128, 128)] = v[64:]
    sub_ = lax.broadcasted_iota(jnp.int32, (8, 128), 0)
    for j in (0, 1):
        tile = offs[0, j]
        for s in (1, 2, 3):
            tile = jnp.where(sub_ < 2 * s, tile, pltpu.roll(offs[s, j], 2 * s, 0))
        m[j] = tile

    sends = []

    def send(src, dst, slot, recv, zd, cd, cond=None):
        same = jnp.logical_and(zd == z, cd == c)
        away = other(same) if cond is None else jnp.logical_and(other(same), cond)
        near_ = same if cond is None else jnp.logical_and(same, cond)
        copy = remote(src, dst, zs.at[slot], recv, z=zd, tp=cd)
        pl.when(near_)(local(src, dst, recv).start)
        pl.when(away)(copy.start)
        sends.append((away, copy))

    odd = lax.rem(z, 2)
    short = gated.at[pl.ds(0, 256), :]
    edge_rows = pl.ds(0, EDGE)

    def part(to):
        return gated.at[pl.ds(pl.multiple_of(to * 256 - EDGE, EDGE), 256 + EDGE), :]

    rows_x = []
    for d in (1, 2, 3):
        to = lax.rem(x + d, 4)
        whole = remote(part(to), gin.at[x], xs.at[d - 1], xr.at[x], x=to)
        less = remote(short, gin.at[x, pl.ds(EDGE, 256), :], xs.at[d - 1], xr.at[x], x=to)
        pl.when(to > 0)(whole.start)
        pl.when(to == 0)(less.start)
        rows_x.append((to, whole, less))
    pl.when(other(first_x))(local(part(x), gin.at[x], xr.at[x]).start)
    pl.when(first_x)(local(short, gin.at[x, pl.ds(EDGE, 256), :], xr.at[x]).start)
    edge = remote(
        gated.at[pl.ds(UNIT - EDGE, EDGE), :], gin.at[x, edge_rows, :], hs.at[0], hr.at[x], z=z + 1, x=0
    )
    pl.when(giver)(edge.start)
    for e in (0, 1, 3, 2):
        jj = lax.rem(z + e, 4)
        zd, j, half = 4 * c + jj, jj // 2, lax.rem(jj, 2)
        for cd in (0, 1):
            q4 = 2 * half + cd
            send(qt.at[j, q4 + odd * (3 - 2 * q4)], qin.at[z], 6 * e + 2 + cd, qs.at[z], zd, cd)
            send(m.at[j], min_.at[z], 6 * e + 4 + cd, ms.at[z], zd, cd)
        send(kp.at[j], kin.at[z], 6 * e, ks.at[z], zd, 0, here if e == 0 else None)
        send(vt.at[j], vin.at[z], 6 * e + 1, vs.at[z], zd, 1, here if e == 0 else None)
    ring_y = Ring("fs", y, lambda b, h: wout.at[b, h], ys, yr)
    ring_y.start()

    @pl.when(jnp.logical_and(first_x, z == 0))
    def _():
        for s in range(4):
            gin[s, edge_rows, :] = jnp.zeros((EDGE, 128), BF16)

    for s in range(4):
        pl.when(other(first_x))(local(part(1), gin.at[s], xr.at[s]).wait)
        pl.when(first_x)(local(short, gin.at[s, pl.ds(EDGE, 256), :], xr.at[s]).wait)
        pl.when(heir)(local(gated.at[edge_rows, :], gin.at[s, edge_rows, :], hr.at[s]).wait)
    for s in range(4):
        ext[s] = gin[s].astype(F32)
    for s in range(4):
        cols = pl.ds(s * 128, 128)

        def block(i, _, s=s, cols=cols):
            at = pl.multiple_of(i * 32, 32)
            total = jnp.zeros((32, 128), F32)
            for tap in range(KW):
                total = total + taps[pl.ds(tap, 1), cols] * ext[s, pl.ds(at + EDGE - (KW - 1) + tap, 32), :]
            rows = pl.ds(at, 32)
            csum[rows, cols] = total
            square = total * total
            if s > 0:
                total = total + stat[0, rows, :]
                square = square + stat[1, rows, :]
            if s == 3:
                total = jnp.broadcast_to(jnp.sum(total, axis=1, keepdims=True), (32, 128))
                square = jnp.broadcast_to(jnp.sum(square, axis=1, keepdims=True), (32, 128))
            stat[0, rows, :] = total
            stat[1, rows, :] = square
            return 0

        lax.fori_loop(0, 8, block, 0)

    zero = jnp.zeros((HD, QB), BF16)
    ones = (lax.broadcasted_iota(jnp.int32, (HD, QB), 0) < 2).astype(F32).astype(BF16)
    col = lax.broadcasted_iota(jnp.int32, (8, 128), 1)

    def pass_on(at, source):
        ref, sem = (kin, ks) if at == 0 else (vin, vs)
        return remote(ref.at[source], ref.at[source], ds.at[source], sem.at[source], tp=1 - at)

    opposite = lax.rem(partner + 4, 8)

    def hand_on(at):
        ref, sem = (kin, ks) if at == 0 else (vin, vs)
        return remote(ref.at[opposite], ref.at[opposite], fs.at[0], sem.at[opposite], z=partner)

    def share(n):
        source = lax.rem(z + nth(n), 8)
        for core in (0, 1):
            @pl.when(c == core)
            def _(core=core):
                copy = pass_on(core, source)
                copy.wait_recv()
                pl.when(source == opposite)(hand_on(core).start)
                copy.start()

    def arrive(n):
        source = lax.rem(z + nth(n), 8)
        pl.when(n < NZ - 1)(lambda: share(n + 1))
        pl.when(n == 3)(ring_y.forward)
        local(qt.at[0, 0], qin.at[source], qs.at[source]).wait()
        local(m.at[0], min_.at[source], ms.at[source]).wait()
        q = qin[source].astype(F32) * (HD**-0.5 * LOG2E)
        high = q.astype(BF16)
        qa[source] = jnp.concatenate([high, ones, (q - high.astype(F32)).astype(BF16), zero], axis=0)
        for core in (0, 1):
            pl.when(c == core)(lambda core=core: pass_on(1 - core, source).wait_recv())
        tile = min_[source] * LOG2E
        for i in range(32):
            packed = kin[source, pl.ds(i * 16, 16), :].astype(F32)
            for first in (0, 64):
                both = []
                for k in (0, 1):
                    at = first + 2 * i + k
                    value = jnp.broadcast_to(tile[:, at : at + 1], (8, 128))
                    top = value.astype(BF16).astype(F32)
                    key = packed[8 * k : 8 * k + 8]
                    key = pltpu.roll(key, 64, 1) if first else key
                    extra = jnp.where(col == HD, top, jnp.where(col == HD + 1, value - top, 0.0))
                    both.append(jnp.where(col < HD, key, extra))
                keys_in[source, pl.ds(first * 8 + i * 16, 16), :] = jnp.concatenate(both, axis=0).astype(BF16)

    def where_is(u):
        one, two = lax.rem(z + nth(u[0]), 8), lax.rem(z + nth(u[1]), 8)
        return jnp.maximum(one, two), jnp.minimum(one, two)

    def following(u):
        n, k = u
        ends = k == n
        return (jnp.where(ends, n + 1, n), jnp.where(ends, 0, k + 1))

    def ready(u):
        pl.when(jnp.logical_and(u[1] == 0, u[0] < NZ))(lambda: arrive(u[0]))

    def scores(u, e_ref, r_ref, t_ref):
        zq, zk = where_is((jnp.minimum(u[0], NZ - 1), u[1]))
        keys_ = keys_in[zk]
        score = jnp.dot(jnp.concatenate([keys_, keys_], axis=1), qa[zq], preferred_element_type=F32)
        which = jnp.where(zq == zk, 1 + lax.rem(zq, 2), 0)
        keep(score, cap.at[which], e_ref, r_ref, t_ref)

    def weights_of(u, e_ref, r_ref, t_ref, w_ref):
        zq, zk = where_is(u)
        weigh(e_ref, r_ref, t_ref, w_ref, left.at[zq * NZ + zk])

    def values(u, w_ref):
        zq, zk = where_is(u)
        acc[zq * NZ + zk] = jnp.dot(vin[zk], w_ref[...], preferred_element_type=F32)

    def combine(zq):
        total = acc[zq * NZ + zq].reshape(8, 8, QB)
        rest = left[zq * NZ + zq]
        for zk in range(zq - 1, -1, -1):
            total = total + acc[zq * NZ + zk].reshape(8, 8, QB) * rest[None]
            if zk > 0:
                rest = rest * left[zq * NZ + zk]
        oout[zq] = total.reshape(HD, QB).astype(BF16)

    across_z = lax.rem(z + 4, 8)

    def give(when):
        for zq in range(NZ):
            pl.when(when(zq))(lambda zq=zq: combine(zq))
        for self_, copy, zq in backs:
            pl.when(jnp.logical_and(other(self_), when(zq)))(copy.start)
            own = local(oout.at[zq], oin.at[head], or_.at[head])
            pl.when(jnp.logical_and(self_, when(zq)))(own.start)

    start = jnp.int32(0)
    w1[...] = jnp.zeros_like(w1)
    share(start)
    ready((start, start))
    scores((start, start), e0, r0, t0)
    remote(stat, stat_in, ss.at[0], sr.at[0], tp=1 - c).start()

    def pair(p, state):
        before, now = state
        pl.when(p == NZ * NZ // 4 - 1)(lambda: give(lambda zq: zq < across_z))
        after = following(now)
        last = following(after)
        ready(after)
        ready(last)
        scores(after, e1, r1, t1)
        weights_of(now, e0, r0, t0, w0)
        values(before, w1)
        scores(last, e0, r0, t0)
        weights_of(after, e1, r1, t1, w1)
        values(now, w0)
        return (after, last)

    last, _ = lax.fori_loop(0, NZ * (NZ + 1) // 4, pair, ((start, start), (start, start)))
    values(last, w1)
    give(lambda zq: zq >= across_z)

    remote(stat, stat_in, ss.at[0], sr.at[0], tp=1 - c).wait()

    def finish(i, _):
        rows = pl.ds(pl.multiple_of(i * 32, 32), 32)
        mean = (stat[0, rows, :] + stat_in[0, rows, :]) / CC
        spread = (stat[1, rows, :] + stat_in[1, rows, :]) / CC - mean * mean
        scale = lax.rsqrt(spread + 1e-06)
        for s in range(4):
            cols = pl.ds(s * 128, 128)
            h = (csum[rows, cols] - mean) * scale * gain[:, cols]
            hidden[rows, cols] = (h / (1.0 + jnp.exp(-h))).astype(BF16)
        return 0

    lax.fori_loop(0, 8, finish, 0)
    ring_y.neighbours()
    ring_y.far()
    for f in range(4):
        conv_part[:, pl.ds(f * 512, 512)] = jnp.dot(hidden[...], wout[f, 1], preferred_element_type=F32)
    for h in range(8):
        local(oout.at[0], oin.at[h], or_.at[h]).wait()
    heads[...] = oin[...].reshape(512, QB).astype(F32).T.astype(BF16)
    theirs, ours = [], []
    for f in range(4):
        cols = pl.ds(f * 512, 512)
        total = jnp.dot(heads[...], wout[f, 0], preferred_element_type=F32)
        total = (total + conv_part[:, cols]).astype(BF16)
        low, high = total[:128], total[128:]
        own_out[:, cols] = jnp.where(c == 0, low, high)
        part_out[:, cols] = jnp.where(c == 0, high, low)
        theirs.append(remote(part_out.at[:, cols], part_in.at[:, cols], ps.at[f], pr.at[f], tp=1 - c))
        ours.append(local(own_out.at[:, cols], own_part.at[:, cols], po.at[f]))
        if f > 0:
            theirs[f - 1].start()
            ours[f - 1].start()
    theirs[3].start()
    ours[3].start()
    for copy in theirs + ours:
        copy.wait()

    for cond, copy in sends:
        pl.when(cond)(copy.wait_send)
    for to, whole, less in rows_x:
        pl.when(to > 0)(whole.wait_send)
        pl.when(to == 0)(less.wait_send)
    pl.when(giver)(edge.wait_send)
    for self_, copy, zq in backs:
        pl.when(other(self_))(copy.wait_send)
    for core in (0, 1):
        @pl.when(c == core)
        def _(core=core):
            for source in range(NZ):
                pass_on(core, source).wait_send()
            hand_on(core).wait_send()

    ring_y.sent()
    ring_x.sent()
    ring_w.sent()


def layer(tokens, tok_gain, offx, taps, gain, *ws):
    vm = pltpu.VMEM
    return pl.pallas_call(
        layer_kernel,
        out_shape=(jax.ShapeDtypeStruct((128, 2048), BF16),) * 2,
        in_specs=[VM] * 5 + [HBM] * 7,
        out_specs=(HBM, HBM),
        scratch_shapes=[
            vm((NX, 2, 128, 2048), BF16),
            vm((4, 512, 640), BF16),
            vm((NX, 2, 8, 128), F32),
            vm((UNIT, 640), F32),
            vm((UNIT, 128), F32),
            vm((UNIT, 128), F32),
            vm((UNIT, 128), F32),
            vm((2, 4, HD, QB), BF16),
            vm((2, 512, 128), BF16),
            vm((2, HD, UNIT), BF16),
            vm((2, 8, 128), F32),
            vm((UNIT, 128), BF16),
            vm((NZ, 512, 128), BF16),
            vm((NZ, HD, UNIT), BF16),
            vm((NZ, HD, QB), BF16),
            vm((NZ, 8, 128), F32),
            vm((NX, 256 + EDGE, 128), BF16),
            vm((4, 2, 512, 512), BF16),
            vm((NX, 256 + EDGE, 128), F32),
            vm((256, 512), F32),
            vm((2, 256, 128), F32),
            vm((2, 256, 128), F32),
            vm((256, 512), BF16),
            vm((256, 512), BF16),
            vm((128, 2048), BF16),
            vm((128, 2048), BF16),
            vm((256, 2048), F32),
            vm((NZ, 256, QB), BF16),
            vm((NZ, UNIT, 128), BF16),
            vm((UNIT, QB), F32),
            vm((UNIT, QB), F32),
            vm((UNIT, QB), BF16),
            vm((UNIT, QB), BF16),
            vm((256, QB), F32),
            vm((256, QB), F32),
            vm((8, QB), F32),
            vm((8, QB), F32),
            vm((3, UNIT, QB), F32),
            vm((NZ * NZ, 8, QB), F32),
            vm((NZ * NZ, HD, QB), F32),
            vm((NZ, HD, QB), BF16),
            vm((8, HD, QB), BF16),
        ]
        + sems(5, 6, 6, 6, 6, 4, 4, 3, 3)
        + sems(2, 6, 6, 24, 8, 8, 8, 8, 8, 1, 3, 4, 1, 4, 1, 1, 8, 8, 4, 4, 4),
        compiler_params=pltpu.CompilerParams(
            collective_id=1, has_side_effects=True, vmem_limit_bytes=63 * 2**20
        ),
        name="layer",
    )(tokens, tok_gain, offx, taps, gain, *ws)


def shards(
    tokens, norm_gain, w_query, w_key, w_value, w_conv_value, w_conv_gate,
    key_offset, conv_kernel, conv_gain, w_attn_out, w_conv_out,
):
    tile = key_offset.astype(F32).T.reshape(NX, 2, 2, 128)
    tile = jnp.pad(tile, ((0, 0), (0, 0), (0, 6), (0, 0)))
    own, other = layer(
        tokens[0], norm_gain[None], tile, conv_kernel, conv_gain[None],
        w_query, w_key, w_value, w_conv_value, w_conv_gate, w_attn_out, w_conv_out,
    )
    return (own.astype(F32) + other.astype(F32)).astype(BF16)[None]


def solution(mesh):
    view = Mesh(mesh.devices.reshape(NZ, NX, 4, 2), ("z", "x", "fs", "tp"))
    rows = P("fs", ("z", "x", "tp"), None)
    placed = (
        rows, P(), P("fs", "tp"), P("fs", "tp"), P("fs", "tp"), P("fs", "tp"), P("fs", "tp"),
        P(("z", "x"), "tp"), P(None, "tp"), P("tp"), P("tp", "fs"), P("tp", "fs"),
    )
    return jax.shard_map(shards, mesh=view, in_specs=placed, out_specs=rows, check_vma=False)
```

```python
import functools
import math

import jax
import jax.numpy as jnp
from jax import lax
from jax.experimental import pallas as pl
from jax.experimental.pallas import tpu as pltpu
from jax.sharding import Mesh
from jax.sharding import PartitionSpec as P

MESH = pl.DeviceIdType.MESH
F32 = jnp.float32
BF16 = jnp.bfloat16
LOG2E = math.log2(math.e)
TOP = 25.0
HD = 64
CC = 1024
KW = 31
UNIT = 1024
QB = 256
NZ = 8
NX = 4
EDGE = 32
VM = pl.BlockSpec(memory_space=pltpu.VMEM)
HBM = pl.BlockSpec(memory_space=pltpu.HBM)


def sems(*counts):
    return [pltpu.SemaphoreType.DMA((n,)) for n in counts]


def remote(src, dst, send, recv, **to):
    return pltpu.make_async_remote_copy(
        src_ref=src, dst_ref=dst, send_sem=send, recv_sem=recv, device_id=to, device_id_type=MESH
    )


def signal(**to):
    pl.semaphore_signal(
        pltpu.get_barrier_semaphore(), inc=1, device_id=to, device_id_type=MESH
    )


class Ring:
    def __init__(self, axis, me, at, send, recv):
        right, left = lax.rem(me + 1, 4), lax.rem(me + 3, 4)
        self.left, self.right = left, right

        def hop(block, half, slot, to):
            ref = at(block, half)
            return remote(ref, ref, send.at[slot], recv.at[slot], **{axis: to})

        self.first = [hop(me, 0, 0, right), hop(me, 1, 2, left), hop(me, 1, 1, right), hop(me, 0, 3, left)]
        self.second = [hop(left, 0, 4, right), hop(right, 1, 5, left)]

    def start(self):
        for copy in self.first:
            copy.start()

    def forward(self):
        for got, copy in zip(self.first[:2], self.second):
            got.wait_recv()
            copy.start()

    def neighbours(self):
        for copy in self.first[2:]:
            copy.wait_recv()

    def far(self):
        for copy in self.second:
            copy.wait_recv()

    def sent(self):
        for copy in self.first + self.second:
            copy.wait_send()


def suffix(t):
    sub = lax.broadcasted_iota(jnp.int32, t.shape, 0)
    e = jnp.where(sub < 7, pltpu.roll(t, 7, 0), 1.0)
    for step in (1, 2, 4):
        e = e * jnp.where(sub < 8 - step, pltpu.roll(e, 8 - step, 0), 1.0)
    return e


def keep(score, cap, e_ref, r_ref, t_ref):
    t = None
    for g in [n // 2 + 16 * (n % 2) for n in range(32)]:
        d = []
        for j in range(4):
            i = 4 * g + j
            rows = pl.ds(i * 8, 8)
            e = jnp.exp2(jnp.minimum(score[i * 8 : i * 8 + 8], cap[rows, :]))
            e_ref[rows, :] = e
            d.append(e + 1.0)
        r = 1.0 / ((d[0] * d[1]) * (d[2] * d[3]))
        r_ref[pl.ds(g * 8, 8), :] = r
        t = r if t is None else t * r
    t_ref[...] = t


def weigh(e_ref, r_ref, t_ref, w_ref, left):
    t = t_ref[...]
    p = suffix(t)
    left[...] = jnp.broadcast_to((p * t)[0:1, :], p.shape)
    for g in range(31, -1, -1):
        p = p * r_ref[pl.ds(g * 8, 8), :]
        rest, w = p, []
        for j in range(4):
            w.append(e_ref[pl.ds((4 * g + j) * 8, 8), :] * rest)
            rest = rest + w[j]
        w_ref[pl.ds(g * 32, 32), :] = jnp.concatenate(w, axis=0).astype(BF16)


ARRIVAL = (0, 7, 3, 1, 5, 6, 2, 4)


def nth(n):
    d = jnp.int32(ARRIVAL[0])
    for k in range(1, NZ):
        d = jnp.where(n == k, ARRIVAL[k], d)
    return d


def layer_kernel(
    tok, tok_gain, offx, taps, gain, wq, wk, wv, wcv, wcg, wa, wc, own_part, part_in,
    rows, weights, offs, full, kf, vf, vp, qt, kp, vt, m, gated,
    kin, vin, qin, min_, gin, wout, ext, csum, stat, stat_in, hidden, heads, own_out, part_out, conv_part,
    qa, keys_in, e0, e1, w0, w1, r0, r1, t0, t1, cap, left, acc, oout, oin,
    ws, cxs, cxr, cys, cyr, cds, cdr, cos, cor,
    wl, ys, yr, zs, ks, vs, qs, ms, ds, fs, xs, xr, hs, hr, ss, sr, os_, or_, ps, pr, po,
):
    z, x, y, c = (lax.axis_index(n) for n in ("z", "x", "fs", "tp"))
    first_loads = [
        pltpu.make_async_copy(
            w.at[:, pl.ds(pl.multiple_of(x * 128, 128), 128)], weights.at[y, :, pl.ds(i * 128, 128)], ws.at[i]
        )
        for i, w in enumerate((wq, wk, wv, wcv, wcg))
    ]
    loads = [pltpu.make_async_copy(w, wout.at[y, i], wl.at[i]) for i, w in enumerate((wa, wc))]
    for load in first_loads:
        load.start()
    home = z // 4
    here = home == c
    other = jnp.logical_not
    local = pltpu.make_async_copy
    for d in range(8):
        if d == 0:
            pl.when(other(here))(lambda: signal(tp=1 - c))
        else:
            signal(z=lax.rem(z + d, 8), tp=home)
    partner = z + 1 - 2 * lax.rem(z, 2)
    signal(tp=1 - c)
    signal(z=partner)
    for d in (1, 2, 3):
        signal(x=lax.rem(x + d, 4))
    signal(fs=lax.rem(y + 1, 4))
    signal(fs=lax.rem(y + 3, 4))
    first_x = x == 0
    heir = jnp.logical_and(first_x, z > 0)
    giver = z < 7

    @pl.when(heir)
    def _():
        for s in range(4):
            signal(z=z - 1, x=s)

    quarter = 2 * lax.rem(z, 2) + c
    head = 2 * x + lax.rem(z // 2, 2)
    wanted = x + lax.rem(z, 2) * (3 - 2 * x)
    for h in range(8):
        zh, xh, ch = 4 * c + 2 * (h % 2) + wanted // 2, h // 2, lax.rem(wanted, 2)
        self_ = jnp.logical_and(jnp.logical_and(zh == z, xh == x), ch == c)
        pl.when(other(self_))(lambda zh=zh, xh=xh, ch=ch: signal(z=zh, x=xh, tp=ch))
    backs = []
    mine = jnp.int32(0)
    for zq in range(NZ):
        xd = quarter if zq % 2 == 0 else 3 - quarter
        self_ = jnp.logical_and(jnp.logical_and(z == zq, xd == x), here)
        mine = mine + self_.astype(jnp.int32)
        copy = remote(oout.at[zq], oin.at[head], os_.at[zq], or_.at[head], z=zq, x=xd, tp=home)
        backs.append((self_, copy, zq))

    def norm(i, _):
        at = pl.ds(pl.multiple_of(i * 16, 16), 16)
        floats = tok[at, :].astype(F32)
        scale = lax.rsqrt(jnp.mean(floats * floats, axis=1, keepdims=True) + 1e-06)
        rows[x, c, at, :] = (floats * scale * tok_gain[...]).astype(BF16)
        return 0

    for load in first_loads:
        load.wait()
    pl.semaphore_wait(
        pltpu.get_barrier_semaphore(),
        23 - here.astype(jnp.int32) + giver.astype(jnp.int32) - mine,
    )

    ring_w = Ring("fs", y, lambda b, h: weights.at[b, pl.ds(h * 256, 256)], cys, cyr)
    ring_x = Ring("x", x, lambda b, h: rows.at[b, c, pl.ds(h * 64, 64)], cxs, cxr)

    def over(block, slot):
        ref = rows.at[block, c]
        return remote(ref, ref, cds.at[slot], cdr.at[slot], tp=1 - c)

    across = [over(x, 0), over(ring_x.left, 1), over(ring_x.right, 2), over(lax.rem(x + 2, 4), 3)]
    ring_w.start()
    lax.fori_loop(0, 8, norm, 0, unroll=4)
    offs[x] = offx[x]
    ring_x.start()
    across[0].start()
    for load in loads:
        load.start()
    small = [
        remote(offx.at[lax.rem(x + d, 4)], offs.at[x], cos.at[d - 1], cor.at[d - 1], x=lax.rem(x + d, 4))
        for d in (1, 2, 3)
    ]
    for copy in small:
        copy.start()
    lane = lax.broadcasted_iota(jnp.int32, (8, QB), 1)
    sub = lax.broadcasted_iota(jnp.int32, (8, QB), 0)

    def caps(i, _):
        key = sub * 128 + i
        rows = pl.ds(pl.multiple_of(i * 8, 8), 8)
        cap[0, rows, :] = jnp.full((8, QB), TOP, F32)
        cap[1, rows, :] = jnp.where(key < lane + quarter * QB, TOP, -300.0)
        cap[2, rows, :] = jnp.where(key < lane + (3 - quarter) * QB, TOP, -300.0)
        return 0

    lax.fori_loop(0, 128, caps, 0, unroll=4)
    ring_x.forward()
    ring_w.forward()
    ring_x.neighbours()
    across[1].start()
    across[2].start()
    for load in loads:
        load.wait()
    ring_w.neighbours()

    def near(b):
        at = pl.ds(pl.multiple_of(b * 256, 256), 256)
        total = None
        for f in (y, ring_w.left, ring_w.right):
            cols = pl.ds(pl.multiple_of(f * 512, 512), 512)
            lhs = jnp.concatenate([rows[b, 0, :, cols], rows[b, 1, :, cols]], axis=0)
            part = jnp.dot(lhs, weights[f], preferred_element_type=F32)
            total = part if total is None else total + part
        full[at, :] = total

    across[0].wait()
    near(x)
    across[1].wait()
    near(ring_x.left)
    ring_x.far()
    across[3].start()
    across[2].wait()
    near(ring_x.right)
    for copy in small:
        copy.wait()
    across[3].wait()
    near(lax.rem(x + 2, 4))
    ring_w.far()
    far = lax.rem(y + 2, 4)

    def block(b, _):
        at = pl.ds(pl.multiple_of(b * 256, 256), 256)
        cols = pl.ds(pl.multiple_of(far * 512, 512), 512)
        lhs = jnp.concatenate([rows[b, 0, :, cols], rows[b, 1, :, cols]], axis=0)
        total = full[at, :] + jnp.dot(lhs, weights[far], preferred_element_type=F32)
        kf[at, :] = total[:, 128:256]
        vf[at, :] = total[:, 256:384]
        q = total[:, :128].T
        qt[0, b] = q[:64].astype(BF16)
        qt[1, b] = q[64:].astype(BF16)
        value = total[:, 384:512].astype(BF16).astype(F32)
        gate = total[:, 512:640].astype(BF16).astype(F32)
        gated[at, :] = (value / (1.0 + jnp.exp(-gate))).astype(BF16)
        return 0

    lax.fori_loop(0, 4, block, 0)
    low = lax.broadcasted_iota(jnp.int32, (8, 128), 1) < 64

    def keys(i, _):
        packed = [[], []]
        for s in (0, 1):
            near_ = kf[pl.ds(2 * i + s, 8, stride=128), :]
            later = kf[pl.ds(2 * i + s + 64, 8, stride=128), :]
            packed[0].append(jnp.where(low, near_, pltpu.roll(later, 64, 1)))
            packed[1].append(jnp.where(low, pltpu.roll(near_, 64, 1), later))
        at = pl.ds(pl.multiple_of(i * 16, 16), 16)
        for j in (0, 1):
            kp[j, at, :] = jnp.concatenate(packed[j], axis=0).astype(BF16)
        return 0

    lax.fori_loop(0, 32, keys, 0, unroll=4)

    def ordered(i, _):
        vp[pl.ds(pl.multiple_of(i * 8, 8), 8), :] = vf[pl.ds(i, 8, stride=128), :]
        return 0

    lax.fori_loop(0, 128, ordered, 0, unroll=8)
    for b in range(8):
        v = vp[pl.ds(b * 128, 128), :].T.astype(BF16)
        vt[0, :, pl.ds(b * 128, 128)] = v[:64]
        vt[1, :, pl.ds(b * 128, 128)] = v[64:]
    sub_ = lax.broadcasted_iota(jnp.int32, (8, 128), 0)
    for j in (0, 1):
        tile = offs[0, j]
        for s in (1, 2, 3):
            tile = jnp.where(sub_ < 2 * s, tile, pltpu.roll(offs[s, j], 2 * s, 0))
        m[j] = tile

    sends = []

    def send(src, dst, slot, recv, zd, cd, cond=None):
        same = jnp.logical_and(zd == z, cd == c)
        away = other(same) if cond is None else jnp.logical_and(other(same), cond)
        near_ = same if cond is None else jnp.logical_and(same, cond)
        copy = remote(src, dst, zs.at[slot], recv, z=zd, tp=cd)
        pl.when(near_)(local(src, dst, recv).start)
        pl.when(away)(copy.start)
        sends.append((away, copy))

    odd = lax.rem(z, 2)
    short = gated.at[pl.ds(0, 256), :]
    edge_rows = pl.ds(0, EDGE)

    def part(to):
        return gated.at[pl.ds(pl.multiple_of(to * 256 - EDGE, EDGE), 256 + EDGE), :]

    rows_x = []
    for d in (1, 2, 3):
        to = lax.rem(x + d, 4)
        whole = remote(part(to), gin.at[x], xs.at[d - 1], xr.at[x], x=to)
        less = remote(short, gin.at[x, pl.ds(EDGE, 256), :], xs.at[d - 1], xr.at[x], x=to)
        pl.when(to > 0)(whole.start)
        pl.when(to == 0)(less.start)
        rows_x.append((to, whole, less))
    pl.when(other(first_x))(local(part(x), gin.at[x], xr.at[x]).start)
    pl.when(first_x)(local(short, gin.at[x, pl.ds(EDGE, 256), :], xr.at[x]).start)
    edge = remote(
        gated.at[pl.ds(UNIT - EDGE, EDGE), :], gin.at[x, edge_rows, :], hs.at[0], hr.at[x], z=z + 1, x=0
    )
    pl.when(giver)(edge.start)
    for e in (0, 1, 3, 2):
        jj = lax.rem(z + e, 4)
        zd, j, half = 4 * c + jj, jj // 2, lax.rem(jj, 2)
        for cd in (0, 1):
            q4 = 2 * half + cd
            send(qt.at[j, q4 + odd * (3 - 2 * q4)], qin.at[z], 6 * e + 2 + cd, qs.at[z], zd, cd)
            send(m.at[j], min_.at[z], 6 * e + 4 + cd, ms.at[z], zd, cd)
        send(kp.at[j], kin.at[z], 6 * e, ks.at[z], zd, 0, here if e == 0 else None)
        send(vt.at[j], vin.at[z], 6 * e + 1, vs.at[z], zd, 1, here if e == 0 else None)
    ring_y = Ring("fs", y, lambda b, h: wout.at[b, h], ys, yr)
    ring_y.start()

    @pl.when(jnp.logical_and(first_x, z == 0))
    def _():
        for s in range(4):
            gin[s, edge_rows, :] = jnp.zeros((EDGE, 128), BF16)

    for s in range(4):
        pl.when(other(first_x))(local(part(1), gin.at[s], xr.at[s]).wait)
        pl.when(first_x)(local(short, gin.at[s, pl.ds(EDGE, 256), :], xr.at[s]).wait)
        pl.when(heir)(local(gated.at[edge_rows, :], gin.at[s, edge_rows, :], hr.at[s]).wait)
    for s in range(4):
        ext[s] = gin[s].astype(F32)
    for s in range(4):
        cols = pl.ds(s * 128, 128)

        def block(i, _, s=s, cols=cols):
            at = pl.multiple_of(i * 32, 32)
            total = jnp.zeros((32, 128), F32)
            for tap in range(KW):
                total = total + taps[pl.ds(tap, 1), cols] * ext[s, pl.ds(at + EDGE - (KW - 1) + tap, 32), :]
            rows = pl.ds(at, 32)
            csum[rows, cols] = total
            square = total * total
            if s > 0:
                total = total + stat[0, rows, :]
                square = square + stat[1, rows, :]
            if s == 3:
                total = jnp.broadcast_to(jnp.sum(total, axis=1, keepdims=True), (32, 128))
                square = jnp.broadcast_to(jnp.sum(square, axis=1, keepdims=True), (32, 128))
            stat[0, rows, :] = total
            stat[1, rows, :] = square
            return 0

        lax.fori_loop(0, 8, block, 0)

    zero = jnp.zeros((HD, QB), BF16)
    ones = (lax.broadcasted_iota(jnp.int32, (HD, QB), 0) < 2).astype(F32).astype(BF16)
    col = lax.broadcasted_iota(jnp.int32, (8, 128), 1)

    def pass_on(at, source):
        ref, sem = (kin, ks) if at == 0 else (vin, vs)
        return remote(ref.at[source], ref.at[source], ds.at[source], sem.at[source], tp=1 - at)

    opposite = lax.rem(partner + 4, 8)

    def hand_on(at):
        ref, sem = (kin, ks) if at == 0 else (vin, vs)
        return remote(ref.at[opposite], ref.at[opposite], fs.at[0], sem.at[opposite], z=partner)

    def share(n):
        source = lax.rem(z + nth(n), 8)
        for core in (0, 1):
            @pl.when(c == core)
            def _(core=core):
                copy = pass_on(core, source)
                copy.wait_recv()
                pl.when(source == opposite)(hand_on(core).start)
                copy.start()

    def arrive(n):
        source = lax.rem(z + nth(n), 8)
        pl.when(n < NZ - 1)(lambda: share(n + 1))
        pl.when(n == 3)(ring_y.forward)
        local(qt.at[0, 0], qin.at[source], qs.at[source]).wait()
        local(m.at[0], min_.at[source], ms.at[source]).wait()
        q = qin[source].astype(F32) * (HD**-0.5 * LOG2E)
        high = q.astype(BF16)
        qa[source] = jnp.concatenate([high, ones, (q - high.astype(F32)).astype(BF16), zero], axis=0)
        for core in (0, 1):
            pl.when(c == core)(lambda core=core: pass_on(1 - core, source).wait_recv())
        tile = min_[source] * LOG2E
        for i in range(32):
            packed = kin[source, pl.ds(i * 16, 16), :].astype(F32)
            for first in (0, 64):
                both = []
                for k in (0, 1):
                    at = first + 2 * i + k
                    value = jnp.broadcast_to(tile[:, at : at + 1], (8, 128))
                    top = value.astype(BF16).astype(F32)
                    key = packed[8 * k : 8 * k + 8]
                    key = pltpu.roll(key, 64, 1) if first else key
                    extra = jnp.where(col == HD, top, jnp.where(col == HD + 1, value - top, 0.0))
                    both.append(jnp.where(col < HD, key, extra))
                keys_in[source, pl.ds(first * 8 + i * 16, 16), :] = jnp.concatenate(both, axis=0).astype(BF16)

    def where_is(u):
        one, two = lax.rem(z + nth(u[0]), 8), lax.rem(z + nth(u[1]), 8)
        return jnp.maximum(one, two), jnp.minimum(one, two)

    def following(u):
        n, k = u
        ends = k == n
        return (jnp.where(ends, n + 1, n), jnp.where(ends, 0, k + 1))

    def ready(u):
        pl.when(jnp.logical_and(u[1] == 0, u[0] < NZ))(lambda: arrive(u[0]))

    def scores(u, e_ref, r_ref, t_ref):
        zq, zk = where_is((jnp.minimum(u[0], NZ - 1), u[1]))
        keys_ = keys_in[zk]
        score = jnp.dot(jnp.concatenate([keys_, keys_], axis=1), qa[zq], preferred_element_type=F32)
        which = jnp.where(zq == zk, 1 + lax.rem(zq, 2), 0)
        keep(score, cap.at[which], e_ref, r_ref, t_ref)

    def weights_of(u, e_ref, r_ref, t_ref, w_ref):
        zq, zk = where_is(u)
        weigh(e_ref, r_ref, t_ref, w_ref, left.at[zq * NZ + zk])

    def values(u, w_ref):
        zq, zk = where_is(u)
        acc[zq * NZ + zk] = jnp.dot(vin[zk], w_ref[...], preferred_element_type=F32)

    def combine(zq):
        total = acc[zq * NZ + zq].reshape(8, 8, QB)
        rest = left[zq * NZ + zq]
        for zk in range(zq - 1, -1, -1):
            total = total + acc[zq * NZ + zk].reshape(8, 8, QB) * rest[None]
            if zk > 0:
                rest = rest * left[zq * NZ + zk]
        oout[zq] = total.reshape(HD, QB).astype(BF16)

    across_z = lax.rem(z + 4, 8)

    def give(when):
        for zq in range(NZ):
            pl.when(when(zq))(lambda zq=zq: combine(zq))
        for self_, copy, zq in backs:
            pl.when(jnp.logical_and(other(self_), when(zq)))(copy.start)
            own = local(oout.at[zq], oin.at[head], or_.at[head])
            pl.when(jnp.logical_and(self_, when(zq)))(own.start)

    start = jnp.int32(0)
    w1[...] = jnp.zeros_like(w1)
    share(start)
    ready((start, start))
    scores((start, start), e0, r0, t0)
    remote(stat, stat_in, ss.at[0], sr.at[0], tp=1 - c).start()

    def pair(p, state):
        before, now = state
        pl.when(p == NZ * NZ // 4 - 1)(lambda: give(lambda zq: zq < across_z))
        after = following(now)
        last = following(after)
        ready(after)
        ready(last)
        scores(after, e1, r1, t1)
        weights_of(now, e0, r0, t0, w0)
        values(before, w1)
        scores(last, e0, r0, t0)
        weights_of(after, e1, r1, t1, w1)
        values(now, w0)
        return (after, last)

    last, _ = lax.fori_loop(0, NZ * (NZ + 1) // 4, pair, ((start, start), (start, start)))
    values(last, w1)
    give(lambda zq: zq >= across_z)

    remote(stat, stat_in, ss.at[0], sr.at[0], tp=1 - c).wait()

    def finish(i, _):
        rows = pl.ds(pl.multiple_of(i * 32, 32), 32)
        mean = (stat[0, rows, :] + stat_in[0, rows, :]) / CC
        spread = (stat[1, rows, :] + stat_in[1, rows, :]) / CC - mean * mean
        scale = lax.rsqrt(spread + 1e-06)
        for s in range(4):
            cols = pl.ds(s * 128, 128)
            h = (csum[rows, cols] - mean) * scale * gain[:, cols]
            hidden[rows, cols] = (h / (1.0 + jnp.exp(-h))).astype(BF16)
        return 0

    lax.fori_loop(0, 8, finish, 0)
    ring_y.neighbours()
    ring_y.far()
    for f in range(4):
        conv_part[:, pl.ds(f * 512, 512)] = jnp.dot(hidden[...], wout[f, 1], preferred_element_type=F32)
    for h in range(8):
        local(oout.at[0], oin.at[h], or_.at[h]).wait()
    heads[...] = oin[...].reshape(512, QB).astype(F32).T.astype(BF16)
    theirs, ours = [], []
    for f in range(4):
        cols = pl.ds(f * 512, 512)
        total = jnp.dot(heads[...], wout[f, 0], preferred_element_type=F32)
        total = (total + conv_part[:, cols]).astype(BF16)
        low, high = total[:128], total[128:]
        own_out[:, cols] = jnp.where(c == 0, low, high)
        part_out[:, cols] = jnp.where(c == 0, high, low)
        theirs.append(remote(part_out.at[:, cols], part_in.at[:, cols], ps.at[f], pr.at[f], tp=1 - c))
        ours.append(local(own_out.at[:, cols], own_part.at[:, cols], po.at[f]))
        if f > 0:
            theirs[f - 1].start()
            ours[f - 1].start()
    theirs[3].start()
    ours[3].start()
    for copy in theirs + ours:
        copy.wait()

    for cond, copy in sends:
        pl.when(cond)(copy.wait_send)
    for to, whole, less in rows_x:
        pl.when(to > 0)(whole.wait_send)
        pl.when(to == 0)(less.wait_send)
    pl.when(giver)(edge.wait_send)
    for self_, copy, zq in backs:
        pl.when(other(self_))(copy.wait_send)
    for core in (0, 1):
        @pl.when(c == core)
        def _(core=core):
            for source in range(NZ):
                pass_on(core, source).wait_send()
            hand_on(core).wait_send()

    ring_y.sent()
    ring_x.sent()
    ring_w.sent()


def layer(tokens, tok_gain, offx, taps, gain, *ws):
    vm = pltpu.VMEM
    return pl.pallas_call(
        layer_kernel,
        out_shape=(jax.ShapeDtypeStruct((128, 2048), BF16),) * 2,
        in_specs=[VM] * 5 + [HBM] * 7,
        out_specs=(HBM, HBM),
        scratch_shapes=[
            vm((NX, 2, 128, 2048), BF16),
            vm((4, 512, 640), BF16),
            vm((NX, 2, 8, 128), F32),
            vm((UNIT, 640), F32),
            vm((UNIT, 128), F32),
            vm((UNIT, 128), F32),
            vm((UNIT, 128), F32),
            vm((2, 4, HD, QB), BF16),
            vm((2, 512, 128), BF16),
            vm((2, HD, UNIT), BF16),
            vm((2, 8, 128), F32),
            vm((UNIT, 128), BF16),
            vm((NZ, 512, 128), BF16),
            vm((NZ, HD, UNIT), BF16),
            vm((NZ, HD, QB), BF16),
            vm((NZ, 8, 128), F32),
            vm((NX, 256 + EDGE, 128), BF16),
            vm((4, 2, 512, 512), BF16),
            vm((NX, 256 + EDGE, 128), F32),
            vm((256, 512), F32),
            vm((2, 256, 128), F32),
            vm((2, 256, 128), F32),
            vm((256, 512), BF16),
            vm((256, 512), BF16),
            vm((128, 2048), BF16),
            vm((128, 2048), BF16),
            vm((256, 2048), F32),
            vm((NZ, 256, QB), BF16),
            vm((NZ, UNIT, 128), BF16),
            vm((UNIT, QB), F32),
            vm((UNIT, QB), F32),
            vm((UNIT, QB), BF16),
            vm((UNIT, QB), BF16),
            vm((256, QB), F32),
            vm((256, QB), F32),
            vm((8, QB), F32),
            vm((8, QB), F32),
            vm((3, UNIT, QB), F32),
            vm((NZ * NZ, 8, QB), F32),
            vm((NZ * NZ, HD, QB), F32),
            vm((NZ, HD, QB), BF16),
            vm((8, HD, QB), BF16),
        ]
        + sems(5, 6, 6, 6, 6, 4, 4, 3, 3)
        + sems(2, 6, 6, 24, 8, 8, 8, 8, 8, 1, 3, 4, 1, 4, 1, 1, 8, 8, 4, 4, 4),
        compiler_params=pltpu.CompilerParams(
            collective_id=1, has_side_effects=True, vmem_limit_bytes=63 * 2**20
        ),
        name="layer",
    )(tokens, tok_gain, offx, taps, gain, *ws)


def shards(
    tokens, norm_gain, w_query, w_key, w_value, w_conv_value, w_conv_gate,
    key_offset, conv_kernel, conv_gain, w_attn_out, w_conv_out,
):
    tile = key_offset.astype(F32).T.reshape(NX, 2, 2, 128)
    tile = jnp.pad(tile, ((0, 0), (0, 0), (0, 6), (0, 0)))
    own, other = layer(
        tokens[0], norm_gain[None], tile, conv_kernel, conv_gain[None],
        w_query, w_key, w_value, w_conv_value, w_conv_gate, w_attn_out, w_conv_out,
    )
    return (own.astype(F32) + other.astype(F32)).astype(BF16)[None]


def solution(mesh):
    view = Mesh(mesh.devices.reshape(NZ, NX, 4, 2), ("z", "x", "fs", "tp"))
    rows = P("fs", ("z", "x", "tp"), None)
    placed = (
        rows, P(), P("fs", "tp"), P("fs", "tp"), P("fs", "tp"), P("fs", "tp"), P("fs", "tp"),
        P(("z", "x"), "tp"), P(None, "tp"), P("tp"), P("tp", "fs"), P("tp", "fs"),
    )
    return jax.shard_map(shards, mesh=view, in_specs=placed, out_specs=rows, check_vma=False)
```
